512 devices in a mesh: grp: 2 (over y), kv: 32 (over z), tp: 8 (over x, core).
Axes of the slice: x: 4, y: 2, z: 32, core: 2. Of those that a mesh axis runs over, the one named last changes fastest.
The devices are a block of a 4x8x32 slice.
Arguments:
- tokens: bfloat16 [256, 2048], P('grp', ('kv', 'tp')), parts along dimension 0, may hold values from -13 to 13, as said below
- state: float32 [256, 16, 128, 128], P(('grp', 'kv'), 'tp'), parts along dimension 0, may hold values from -0.6 to 0.6
- norm_gain: bfloat16 [2048], P('kv'), may hold values from 0.099609375 to 1.8984375
- w_query: bfloat16 [2048, 2048], P('kv', 'tp'), may hold values from -0.125 to 0.125
- w_key: bfloat16 [2048, 2048], P('kv', 'tp'), may hold values from -0.125 to 0.125
- w_value: bfloat16 [2048, 2048], P('kv', 'tp'), may hold values from -0.125 to 0.125
- w_beta: bfloat16 [2048, 16], replicated, may hold values from -0.125 to 0.125
- w_decay: bfloat16 [2048, 16], replicated, may hold values from -0.125 to 0.125
- a_log: float32 [16], P('tp'), may hold values from -3 to 1
- dt_bias: float32 [16], P('tp'), may hold values from -2 to 1
- head_gain: float32 [128], replicated, may hold values from 0.1 to 1.9
- w_out: bfloat16 [2048, 2048], P('tp', 'kv'), may hold values from -0.125 to 0.125
- mixer_gain: bfloat16 [2048], P('kv'), may hold values from 0.099609375 to 1.8984375
- w_up: bfloat16 [2048, 8192], P('kv', 'tp'), may hold values from -0.125 to 0.125
- w_down: bfloat16 [8192, 2048], P('tp', 'kv'), may hold values from -0.0625 to 0.0625
Outputs:
- mixed: bfloat16 [256, 2048], P('grp', ('kv', 'tp')), parts along dimension 0
- new_state: float32 [256, 16, 128, 128], P(('grp', 'kv'), 'tp'), parts along dimension 0
The draws below stay inside these ranges and needn't reach their ends.
There are 2 independent parts, one for each index of `grp`. The reference program is written for one: setup_inputs(seed, part) draws one part's arguments, and reference() takes and returns one part's arrays. A program takes and returns all parts, laid end to end along the dimension named above; an argument that names none is the same for every part. Nothing has to cross between parts.
Inputs may be any that keep to these rules, and one draw needn't show every extreme that they name: `tokens`: activations of order one.
All inputs are finite; a program needn't handle non-finite values.
Results may differ from the reference program's by a relative error of at most 0.019.
Values may be sent and summed in bfloat16 or wider, within the bound.
No kernel may reach another device: no remote copies, remote signals or barrier semaphores. Data moves between devices by JAX's collectives and lax.ppermute only.
A program may use at most 64 MiB of HBM per device.

```python
import jax
import jax.numpy as jnp
from jax import lax

D = 2048
HEADS = 16
HEAD = 128
FF = 8192
BATCH = 128
N_TP = 8


def draw_tokens(key, part):
    first_key, second_key = jax.random.split(jax.random.fold_in(key, 17), 2)
    ramp = jnp.exp(jnp.linspace(jnp.log(0.5), jnp.log(1.5), D)).astype(jnp.float32)
    rough = jnp.exp(jax.random.uniform(second_key, (1, D), jnp.float32, -0.35, 0.35))
    base = jnp.clip(jax.random.normal(first_key, (BATCH, D), jnp.float32), -6.0, 6.0)
    return (base * ramp * rough).astype(jnp.bfloat16)


def steps_of(rng, extent, shards, low, top_value):
    def one(dim, blocks):
        heights = jax.random.uniform(jax.random.fold_in(jax.random.fold_in(rng, 6), dim), (blocks,), jnp.float32, low / len(shards), top_value / len(shards))
        return jnp.repeat(jnp.exp(heights), extent[dim] // blocks).reshape((-1,) + (1,) * (len(extent) - dim - 1))

    loudness = one(*shards[0])
    for cut in shards[1:]:
        loudness = loudness * one(*cut)
    return loudness


def scatter_about(key, shape, spread, limit, cuts=(), held_as=jnp.bfloat16):
    array = spread * jax.random.normal(key, shape, jnp.float32)
    if cuts:
        array = array * steps_of(key, shape, cuts, -0.22, 0.18)
    return jnp.clip(array, -limit, limit).astype(held_as)


def setup_inputs(seed: int = 0, part: int = 0) -> dict:
    splits = jax.random.split(jax.random.key(seed), 16)
    own_keys = jax.random.split(jax.random.fold_in(splits[15], part), 16)
    tokens = draw_tokens(jax.random.fold_in(jax.random.fold_in(splits[15], part), 71), part)
    state = scatter_about(own_keys[1], (BATCH, HEADS, HEAD, HEAD), 0.1, 0.6, ((0, 32), (1, 8)), jnp.float32)
    norm_gain = jnp.clip(1.0 + 0.18 * jax.random.normal(splits[2], (D,), jnp.float32), 0.099609375, 1.8984375).astype(jnp.bfloat16)
    w_query = scatter_about(splits[3], (D, HEADS * HEAD), D ** -0.5, 0.125, ((0, 32), (1, 8)))
    w_key = scatter_about(splits[4], (D, HEADS * HEAD), D ** -0.5, 0.125, ((0, 32), (1, 8)))
    w_value = scatter_about(splits[5], (D, HEADS * HEAD), D ** -0.5, 0.125, ((0, 32), (1, 8)))
    w_beta = scatter_about(splits[6], (D, HEADS), D ** -0.5, 0.125)
    w_decay = scatter_about(splits[7], (D, HEADS), D ** -0.5, 0.125)
    a_log = jnp.clip(-3.0 + 4.0 * jax.random.uniform(splits[8], (HEADS,), jnp.float32) ** steps_of(splits[8], (HEADS,), ((0, 8),), -0.2, 0.2), -3.0, 1.0)
    dt_bias = jnp.clip(-2.0 + 3.0 * jax.random.uniform(splits[9], (HEADS,), jnp.float32) ** steps_of(splits[9], (HEADS,), ((0, 8),), -0.2, 0.2), -2.0, 1.0)
    head_gain = jnp.clip(1.0 + 0.18 * jax.random.normal(splits[10], (HEAD,), jnp.float32), 0.1, 1.9)
    w_out = scatter_about(splits[11], (HEADS * HEAD, D), (HEADS * HEAD) ** -0.5, 0.125, ((0, 8), (1, 32)))
    mixer_gain = jnp.clip(1.0 + 0.18 * jax.random.normal(splits[12], (D,), jnp.float32), 0.099609375, 1.8984375).astype(jnp.bfloat16)
    w_up = scatter_about(splits[13], (D, FF), D ** -0.5, 0.125, ((0, 32), (1, 8)))
    w_down = scatter_about(splits[14], (FF, D), FF ** -0.5, 0.0625, ((0, 8), (1, 32)))
    return {"tokens": tokens, "state": state, "norm_gain": norm_gain, "w_query": w_query, "w_key": w_key, "w_value": w_value, "w_beta": w_beta, "w_decay": w_decay, "a_log": a_log, "dt_bias": dt_bias, "head_gain": head_gain, "w_out": w_out, "mixer_gain": mixer_gain, "w_up": w_up, "w_down": w_down}


epsilon = 1e-06

def dotted(left, right):
    return jnp.dot(left, right, preferred_element_type=jnp.float32)

def delta_update(query_pre, key_pre, value_pre, beta_pre, decay_pre, state, a_log, dt_bias, head_gain):
    query = query_pre * lax.rsqrt(lax.optimization_barrier(jnp.sum(query_pre * query_pre, axis=-1, keepdims=True)) + epsilon)
    keyed = key_pre * lax.rsqrt(lax.optimization_barrier(jnp.sum(key_pre * key_pre, axis=-1, keepdims=True)) + epsilon)
    beta = jax.nn.sigmoid(beta_pre)
    decay = jnp.exp(-jnp.exp(a_log) * jax.nn.softplus(decay_pre + dt_bias))
    key_read = jnp.einsum('bhk,bhkv->bhv', keyed, state)
    query_read = jnp.einsum('bhk,bhkv->bhv', query, state)
    fresh = beta[..., None] * (value_pre - decay[..., None] * key_read)
    new_state = decay[..., None, None] * state + keyed[..., :, None] * fresh[..., None, :]
    intersection = lax.optimization_barrier(jnp.sum(query * keyed, axis=-1))
    reading = decay[..., None] * query_read + intersection[..., None] * fresh
    normed = reading * lax.rsqrt(lax.optimization_barrier(jnp.mean(reading * reading, axis=-1, keepdims=True)) + epsilon) * head_gain
    return (normed.astype(jnp.bfloat16), new_state)

def grouped_sum(left, weight, groups):
    rows = left.shape[0]
    width = left.shape[1] // groups
    left_g = left.reshape(rows, groups, width).astype(jnp.float32)
    weight_g = weight.reshape(groups, width, weight.shape[1]).astype(jnp.float32)
    partial_g = jnp.einsum('bgi,gio->bgo', left_g, weight_g)
    return lax.optimization_barrier(jnp.sum(partial_g.astype(jnp.bfloat16).astype(jnp.float32), axis=1))

def reference(tokens, state, norm_gain, w_query, w_key, w_value, w_beta, w_decay, a_log, dt_bias, head_gain, w_out, mixer_gain, w_up, w_down):
    rows = tokens.shape[0]
    inputs = tokens.astype(jnp.float32)
    first = lax.rsqrt(lax.optimization_barrier(jnp.mean(inputs * inputs, axis=-1, keepdims=True)) + epsilon)
    scaled = (inputs * norm_gain.astype(jnp.float32)).astype(jnp.bfloat16)
    query_pre = (first * dotted(scaled, w_query)).reshape(rows, HEADS, HEAD)
    key_pre = (first * dotted(scaled, w_key)).reshape(rows, HEADS, HEAD)
    value_pre = (first * dotted(scaled, w_value)).reshape(rows, HEADS, HEAD)
    beta_pre = first * dotted(scaled, w_beta)
    decay_pre = first * dotted(scaled, w_decay)
    normed, new_state = delta_update(query_pre, key_pre, value_pre, beta_pre, decay_pre, state, a_log, dt_bias, head_gain)
    attended = grouped_sum(normed.reshape(rows, HEADS * HEAD), w_out, N_TP)
    middle = (inputs + attended).astype(jnp.bfloat16)
    middle_f = middle.astype(jnp.float32)
    second = lax.rsqrt(lax.optimization_barrier(jnp.mean(middle_f * middle_f, axis=-1, keepdims=True)) + epsilon)
    scaled_two = (middle_f * mixer_gain.astype(jnp.float32)).astype(jnp.bfloat16)
    hidden = jnp.square(jax.nn.relu(second * dotted(scaled_two, w_up))).astype(jnp.bfloat16)
    lowered = grouped_sum(hidden, w_down, N_TP)
    mixed = (middle_f + lowered).astype(jnp.bfloat16)
    return (mixed, new_state)
```

```python
import jax
import jax.numpy as jnp
from jax import lax
from jax.sharding import PartitionSpec as P

epsilon = 1e-06
bf16 = jnp.bfloat16
f32 = jnp.float32


def exchange(x, axis):
    return lax.all_to_all(x, axis, split_axis=0, concat_axis=0, tiled=True)


def from_everyone(x, axis):
    return exchange(jnp.broadcast_to(x, (lax.axis_size(axis), *x.shape)), axis)


def dotted(left, right, left_dim, right_dim):
    dims = (((left_dim,), (right_dim,)), ((), ()))
    return lax.dot_general(left, right, dims, preferred_element_type=f32)


def delta_update(
    query_pre, key_pre, value_pre, beta_pre, decay_pre, state, a_log, dt_bias, head_gain
):
    query = query_pre * lax.rsqrt(jnp.sum(query_pre * query_pre, axis=-1, keepdims=True) + epsilon)
    keyed = key_pre * lax.rsqrt(jnp.sum(key_pre * key_pre, axis=-1, keepdims=True) + epsilon)
    beta = jax.nn.sigmoid(beta_pre)
    decay = jnp.exp(-jnp.exp(a_log) * jax.nn.softplus(decay_pre + dt_bias))
    key_read = jnp.einsum("bhk,bhkv->bhv", keyed, state)
    query_read = jnp.einsum("bhk,bhkv->bhv", query, state)
    fresh = beta[..., None] * (value_pre - decay[..., None] * key_read)
    new_state = decay[..., None, None] * state + keyed[..., :, None] * fresh[..., None, :]
    intersection = jnp.sum(query * keyed, axis=-1)
    reading = decay[..., None] * query_read + intersection[..., None] * fresh
    normed = (
        reading
        * lax.rsqrt(jnp.mean(reading * reading, axis=-1, keepdims=True) + epsilon)
        * head_gain
    )
    return (normed.astype(bf16), new_state)


def mixer_weights(w_up, w_down, mixer_gain, n_kv, n_tp):
    gained = (w_up.astype(f32) * mixer_gain.astype(f32)[:, None]).astype(bf16)
    own = gained.shape[0] // n_tp
    wide = gained.shape[1]
    both = jnp.stack([gained.reshape(n_tp, own, wide), w_down.T.reshape(n_tp, own, wide)], axis=1)
    arrived = exchange(both, "tp")
    hidden_here = wide * n_tp // n_kv
    pieces = arrived.reshape(n_tp, 2, own, wide // hidden_here, hidden_here)
    pieces = pieces.transpose(0, 3, 1, 2, 4).reshape(n_kv, 2, own, hidden_here)
    whole = exchange(pieces, "kv")
    up = whole[:, 0].reshape(n_kv * own, hidden_here)
    down_t = whole[:, 1].reshape(n_kv * own, hidden_here)
    return up, down_t


def local(
    tokens,
    state,
    norm_gain,
    w_query,
    w_key,
    w_value,
    w_beta,
    w_decay,
    a_log,
    dt_bias,
    head_gain,
    w_out,
    mixer_gain,
    w_up,
    w_down,
):
    seq_here, heads_here, head_size = state.shape[:3]
    n_kv = lax.axis_size("kv")
    n_tp = lax.axis_size("tp")
    width = w_beta.shape[0]
    rows, own = tokens.shape
    block = own * n_tp
    kv_index = lax.axis_index("kv")
    tp_index = lax.axis_index("tp")
    columns = heads_here * head_size

    tokens_t = tokens.T
    inputs = from_everyone(tokens_t, "tp").reshape(block, rows).astype(f32)
    scaled = (inputs * norm_gain.astype(f32)[:, None]).astype(bf16)
    squares = jnp.sum(inputs * inputs, axis=0)
    at = (kv_index * block, tp_index * heads_here)
    beta_rows = lax.dynamic_slice(w_beta, at, (block, heads_here))
    decay_rows = lax.dynamic_slice(w_decay, at, (block, heads_here))
    parts = [
        dotted(scaled, w_query, 0, 0).astype(bf16),
        dotted(scaled, w_key, 0, 0).astype(bf16),
        dotted(scaled, w_value, 0, 0).astype(bf16),
        dotted(scaled, jnp.concatenate([beta_rows, decay_rows], axis=1), 0, 0).astype(bf16),
        squares[:, None].astype(bf16),
    ]
    sent = jnp.concatenate(parts, axis=1).reshape(n_kv, seq_here, -1)
    sums = exchange(sent, "kv").astype(f32).sum(axis=0)
    first = lax.rsqrt(sums[:, -1:] / width + epsilon)
    pre = first * sums
    heads = lambda n: pre[:, n * columns : (n + 1) * columns].reshape(seq_here, heads_here, head_size)
    gates = pre[:, 3 * columns :]
    normed, new_state = delta_update(
        heads(0),
        heads(1),
        heads(2),
        gates[:, :heads_here],
        gates[:, heads_here : 2 * heads_here],
        state,
        a_log,
        dt_bias,
        head_gain,
    )
    up, down_t = mixer_weights(w_up, w_down, mixer_gain, n_kv, n_tp)

    every = from_everyone(normed.reshape(seq_here, columns), "kv").reshape(rows, columns)
    head_part = dotted(w_out, every, 0, 1).astype(bf16)
    arrived = exchange(head_part.reshape(n_tp, own, rows), "tp")
    middle_own = (tokens_t.astype(f32) + arrived.astype(f32).sum(axis=0)).astype(bf16)

    middle = from_everyone(middle_own, "kv").reshape(n_kv * own, rows)
    middle_f = middle.astype(f32)
    squares_two = jnp.sum(middle_f * middle_f, axis=0, keepdims=True)
    hidden_part = dotted(up, middle, 0, 0)
    tail = jnp.broadcast_to(squares_two, (8, rows))
    sent = jnp.concatenate([hidden_part, tail], axis=0).astype(bf16)
    sums = from_everyone(sent, "tp").astype(f32).sum(axis=0)
    second = lax.rsqrt(sums[-1:] / width + epsilon)
    hidden = jnp.square(jax.nn.relu(second * sums[:-8])).astype(bf16)
    down_part = dotted(down_t, hidden, 1, 0).astype(bf16)
    lowered = exchange(down_part.reshape(n_kv, own, rows), "kv").astype(f32).sum(axis=0)
    mixed = (middle_own.astype(f32) + lowered).astype(bf16).T
    return (mixed, new_state)


def solution(mesh):
    return jax.shard_map(
        local,
        mesh=mesh,
        in_specs=(
            P("grp", ("kv", "tp")),
            P(("grp", "kv"), "tp", None, None),
            P("kv"),
            P("kv", "tp"),
            P("kv", "tp"),
            P("kv", "tp"),
            P(),
            P(),
            P("tp"),
            P("tp"),
            P(),
            P("tp", "kv"),
            P("kv"),
            P("kv", "tp"),
            P("tp", "kv"),
        ),
        out_specs=(P("grp", ("kv", "tp")), P(("grp", "kv"), "tp", None, None)),
        check_vma=False,
    )
```

```python
import jax
import jax.numpy as jnp
from jax import lax
from jax.sharding import Mesh
from jax.sharding import PartitionSpec as P


epsilon = 1e-06
bf16 = jnp.bfloat16
f32 = jnp.float32
KV = ("hi", "lo")
NEAR = ("lo", "tp")
NEIGHBOURS = 8


def exchange(x, axis):
    return lax.all_to_all(x, axis, split_axis=0, concat_axis=0, tiled=True)


def from_everyone(x, axis):
    return exchange(jnp.broadcast_to(x, (lax.axis_size(axis), *x.shape)), axis)


def dotted(left, right, left_dim, right_dim):
    dims = (((left_dim,), (right_dim,)), ((), ()))
    return lax.dot_general(left, right, dims, preferred_element_type=f32)


def delta_update(
    query_pre, key_pre, value_pre, beta_pre, decay_pre, state, a_log, dt_bias, head_gain
):
    query = query_pre * lax.rsqrt(jnp.sum(query_pre * query_pre, axis=-1, keepdims=True) + epsilon)
    keyed = key_pre * lax.rsqrt(jnp.sum(key_pre * key_pre, axis=-1, keepdims=True) + epsilon)
    beta = jax.nn.sigmoid(beta_pre)
    decay = jnp.exp(-jnp.exp(a_log) * jax.nn.softplus(decay_pre + dt_bias))
    key_read = jnp.einsum("bhk,bhkv->bhv", keyed, state)
    query_read = jnp.einsum("bhk,bhkv->bhv", query, state)
    fresh = beta[..., None] * (value_pre - decay[..., None] * key_read)
    new_state = decay[..., None, None] * state + keyed[..., :, None] * fresh[..., None, :]
    intersection = jnp.sum(query * keyed, axis=-1)
    reading = decay[..., None] * query_read + intersection[..., None] * fresh
    normed = (
        reading
        * lax.rsqrt(jnp.mean(reading * reading, axis=-1, keepdims=True) + epsilon)
        * head_gain
    )
    return (normed.astype(bf16), new_state)


def mixer_weights(w_up, w_down, mixer_gain):
    near = lax.axis_size("lo")
    me = lax.axis_index("lo")
    block, wide = w_up.shape
    share = wide // near
    gained = (w_up.astype(f32) * mixer_gain.astype(f32)[:, None]).astype(bf16)
    both = jnp.concatenate([gained, w_down.T], axis=0)
    both = both.reshape(2 * block, near, share).transpose(1, 0, 2)
    whole = jnp.zeros_like(both)
    for step in range(near):
        piece = lax.dynamic_slice_in_dim(both, me ^ step, 1, axis=0)
        if step:
            piece = lax.ppermute(piece, "lo", [(i, i ^ step) for i in range(near)])
        whole = lax.dynamic_update_slice_in_dim(whole, piece, me ^ step, axis=0)
    up = whole[:, :block].reshape(near * block, share)
    down_t = whole[:, block:].reshape(near * block, share)
    return up, down_t


def local(
    tokens,
    state,
    norm_gain,
    w_query,
    w_key,
    w_value,
    w_beta,
    w_decay,
    a_log,
    dt_bias,
    head_gain,
    w_out,
    mixer_gain,
    w_up,
    w_down,
):
    seq_here, heads_here, head_size = state.shape[:3]
    n_kv = lax.axis_size(KV)
    n_tp = lax.axis_size("tp")
    n_near = lax.axis_size(NEAR)
    width = w_beta.shape[0]
    rows, own = tokens.shape
    block = own * n_tp
    kv_index = lax.axis_index(KV)
    tp_index = lax.axis_index("tp")
    columns = heads_here * head_size

    tokens_t = tokens.T
    inputs = from_everyone(tokens_t, "tp").reshape(block, rows).astype(f32)
    scaled = (inputs * norm_gain.astype(f32)[:, None]).astype(bf16)
    squares = jnp.sum(inputs * inputs, axis=0)
    at = (kv_index * block, tp_index * heads_here)
    beta_rows = lax.dynamic_slice(w_beta, at, (block, heads_here))
    decay_rows = lax.dynamic_slice(w_decay, at, (block, heads_here))
    parts = [
        dotted(scaled, w_query, 0, 0).astype(bf16),
        dotted(scaled, w_key, 0, 0).astype(bf16),
        dotted(scaled, w_value, 0, 0).astype(bf16),
        dotted(scaled, jnp.concatenate([beta_rows, decay_rows], axis=1), 0, 0).astype(bf16),
        squares[:, None].astype(bf16),
    ]
    sent = jnp.concatenate(parts, axis=1).reshape(n_kv, seq_here, -1)
    arrived = exchange(sent, KV)
    sums = arrived.astype(f32).sum(axis=0)
    first = lax.rsqrt(sums[:, -1:] / width + epsilon)
    pre = first * sums
    heads = lambda n: pre[:, n * columns : (n + 1) * columns].reshape(seq_here, heads_here, head_size)
    gates = pre[:, 3 * columns :]
    normed, new_state = delta_update(
        heads(0),
        heads(1),
        heads(2),
        gates[:, :heads_here],
        gates[:, heads_here : 2 * heads_here],
        state,
        a_log,
        dt_bias,
        head_gain,
    )
    up, down_t = mixer_weights(w_up, w_down, mixer_gain)

    every = from_everyone(normed.reshape(seq_here, columns), KV).reshape(rows, columns)
    head_part = dotted(w_out, every, 0, 1).astype(bf16)
    arrived = exchange(head_part.reshape(n_tp, own, rows), "tp")
    middle_own = (tokens_t.astype(f32) + arrived.astype(f32).sum(axis=0)).astype(bf16)

    middle = from_everyone(middle_own, NEAR).reshape(n_near * own, rows)
    middle_f = middle.astype(f32)
    squares_two = jnp.sum(middle_f * middle_f, axis=0, keepdims=True)
    hidden_part = dotted(up, middle, 0, 0)
    tail = jnp.broadcast_to(squares_two, (8, rows))
    sent = jnp.concatenate([hidden_part, tail], axis=0).astype(bf16)
    sums = from_everyone(sent, "hi").astype(f32).sum(axis=0)
    second = lax.rsqrt(sums[-1:] / width + epsilon)
    hidden = jnp.square(jax.nn.relu(second * sums[:-8])).astype(bf16)
    down_part = dotted(down_t, hidden, 1, 0).astype(bf16)
    arrived = exchange(down_part.reshape(n_near, own, rows), NEAR)
    lowered = arrived.astype(f32).sum(axis=0)
    mixed = (middle_own.astype(f32) + lowered).astype(bf16).T
    return (mixed, new_state)


def solution(mesh):
    near = min(NEIGHBOURS, mesh.shape["kv"])
    devices = mesh.devices.reshape(mesh.shape["grp"], -1, near, mesh.shape["tp"])
    fine = Mesh(devices, ("grp", "hi", "lo", "tp"))
    every = ("hi", "lo", "tp")
    return jax.shard_map(
        local,
        mesh=fine,
        in_specs=(
            P("grp", every),
            P(("grp", "hi", "lo"), "tp", None, None),
            P(KV),
            P(KV, "tp"),
            P(KV, "tp"),
            P(KV, "tp"),
            P(),
            P(),
            P("tp"),
            P("tp"),
            P(),
            P("tp", KV),
            P(KV),
            P(KV, "tp"),
            P("tp", KV),
        ),
        out_specs=(P("grp", every), P(("grp", "hi", "lo"), "tp", None, None)),
        check_vma=False,
    )
```

```python
import jax
import jax.numpy as jnp
from jax import lax
from jax.sharding import Mesh
from jax.sharding import PartitionSpec as P


epsilon = 1e-06
bf16 = jnp.bfloat16
f32 = jnp.float32
KV = ("hi", "mid", "pair")
LO = ("mid", "pair")
NEIGHBOURS = 8


def exchange(x, axis):
    return lax.all_to_all(x, axis, split_axis=0, concat_axis=0, tiled=True)


def from_everyone(x, axis):
    return exchange(jnp.broadcast_to(x, (lax.axis_size(axis), *x.shape)), axis)


def dotted(left, right, left_dim, right_dim):
    dims = (((left_dim,), (right_dim,)), ((), ()))
    return lax.dot_general(left, right, dims, preferred_element_type=f32)


def delta_update(
    query_pre, key_pre, value_pre, beta_pre, decay_pre, state, a_log, dt_bias, head_gain
):
    query = query_pre * lax.rsqrt(jnp.sum(query_pre * query_pre, axis=-1, keepdims=True) + epsilon)
    keyed = key_pre * lax.rsqrt(jnp.sum(key_pre * key_pre, axis=-1, keepdims=True) + epsilon)
    beta = jax.nn.sigmoid(beta_pre)
    decay = jnp.exp(-jnp.exp(a_log) * jax.nn.softplus(decay_pre + dt_bias))
    key_read = jnp.einsum("bhk,bhkv->bhv", keyed, state)
    query_read = jnp.einsum("bhk,bhkv->bhv", query, state)
    fresh = beta[..., None] * (value_pre - decay[..., None] * key_read)
    new_state = decay[..., None, None] * state + keyed[..., :, None] * fresh[..., None, :]
    intersection = jnp.sum(query * keyed, axis=-1)
    reading = decay[..., None] * query_read + intersection[..., None] * fresh
    normed = (
        reading
        * lax.rsqrt(jnp.mean(reading * reading, axis=-1, keepdims=True) + epsilon)
        * head_gain
    )
    return (normed.astype(bf16), new_state)


def mixer_weights(w_up, w_down, mixer_gain, n_tp):
    near = lax.axis_size(LO)
    me = lax.axis_index(LO)
    block, wide = w_up.shape
    share = wide // near
    gained = (w_up.astype(f32) * mixer_gain.astype(f32)[:, None]).astype(bf16)
    both = jnp.concatenate([gained, w_down.T], axis=0)
    both = both.reshape(2 * block, near, share).transpose(1, 0, 2)
    whole = jnp.zeros_like(both)
    for step in range(near):
        piece = lax.dynamic_slice_in_dim(both, me ^ step, 1, axis=0)
        if step:
            piece = lax.ppermute(piece, LO, [(i, i ^ step) for i in range(near)])
        whole = lax.dynamic_update_slice_in_dim(whole, piece, me ^ step, axis=0)
    up = whole[:, :block].reshape(near * block, share)
    down_t = whole[:, block:].reshape(near, n_tp, block // n_tp, share)
    down_t = down_t.transpose(1, 0, 2, 3).reshape(near * block, share)
    return up, down_t


def local(
    tokens,
    state,
    norm_gain,
    w_query,
    w_key,
    w_value,
    w_beta,
    w_decay,
    a_log,
    dt_bias,
    head_gain,
    w_out,
    mixer_gain,
    w_up,
    w_down,
):
    seq_here, heads_here, head_size = state.shape[:3]
    n_kv = lax.axis_size(KV)
    n_tp = lax.axis_size("tp")
    n_near = lax.axis_size(LO)
    width = w_beta.shape[0]
    rows, own = tokens.shape
    block = own * n_tp
    kv_index = lax.axis_index(KV)
    tp_index = lax.axis_index("tp")
    side = lax.axis_index("pair")
    columns = heads_here * head_size
    assert heads_here == lax.axis_size("pair")

    tokens_t = tokens.T
    gain = norm_gain.astype(f32)[:, None]
    split = lambda w: w.reshape(block, heads_here, head_size).transpose(1, 0, 2)
    by_head = jnp.concatenate([split(w_query), split(w_key), split(w_value)], axis=2)
    by_head = (by_head.astype(f32) * gain).astype(bf16)
    kept = lax.dynamic_index_in_dim(by_head, side, 0, keepdims=False)
    given = lax.dynamic_index_in_dim(by_head, 1 - side, 0, keepdims=False)
    taken = lax.ppermute(given, "pair", [(0, 1), (1, 0)])

    both = from_everyone(tokens_t, ("pair", "tp")).reshape(2, block, rows)
    mine = lax.dynamic_index_in_dim(both, side, 0, keepdims=False)
    other = lax.dynamic_index_in_dim(both, 1 - side, 0, keepdims=False)
    inputs = mine.astype(f32)
    scaled = (inputs * gain).astype(bf16)
    squares = jnp.sum(inputs * inputs, axis=0)
    at = (kv_index * block, tp_index * heads_here)
    beta_rows = lax.dynamic_slice(w_beta, at, (block, heads_here))
    decay_rows = lax.dynamic_slice(w_decay, at, (block, heads_here))
    parts = [
        (dotted(mine, kept, 0, 0) + dotted(other, taken, 0, 0)).astype(bf16),
        dotted(scaled, jnp.concatenate([beta_rows, decay_rows], axis=1), 0, 0).astype(bf16),
        squares[:, None].astype(bf16),
    ]
    sent = jnp.concatenate(parts, axis=1).reshape(n_kv, seq_here, -1)
    arrived = exchange(sent, KV)
    main = 3 * head_size
    sums = arrived.astype(f32)
    gates = sums[..., main:].sum(axis=0)
    sums = sums[..., :main].reshape(-1, heads_here, seq_here, main).sum(axis=0)
    first = lax.rsqrt(gates[:, -1:] / width + epsilon)
    pre = (first * sums).transpose(1, 0, 2)
    gates = first * gates
    heads = lambda n: pre[..., n * head_size : (n + 1) * head_size]
    normed, new_state = delta_update(
        heads(0),
        heads(1),
        heads(2),
        gates[:, :heads_here],
        gates[:, heads_here : 2 * heads_here],
        state,
        a_log,
        dt_bias,
        head_gain,
    )
    up, down_t = mixer_weights(w_up, w_down, mixer_gain, n_tp)

    every = from_everyone(normed.reshape(seq_here, columns), KV).reshape(rows, columns)
    every, up, down_t, new_state = lax.optimization_barrier((every, up, down_t, new_state))
    head_part = dotted(w_out, every, 0, 1).astype(bf16)
    attended = from_everyone(head_part, "tp").astype(f32).sum(axis=0)
    middle_block = (inputs + attended).astype(bf16)
    middle_own = lax.dynamic_slice_in_dim(middle_block, tp_index * own, own, axis=0)

    middle = from_everyone(middle_block, LO).reshape(n_near * block, rows)
    middle_f = middle.astype(f32)
    squares_two = jnp.sum(middle_f * middle_f, axis=0, keepdims=True)
    hidden_part = dotted(up, middle, 0, 0)
    tail = jnp.broadcast_to(squares_two, (8, rows))
    sent = jnp.concatenate([hidden_part, tail], axis=0).astype(bf16)
    sums = from_everyone(sent, "hi").astype(f32).sum(axis=0)
    second = lax.rsqrt(sums[-1:] / width + epsilon)
    hidden = jnp.square(jax.nn.relu(second * sums[:-8])).astype(bf16)
    down_part = dotted(down_t, hidden, 1, 0).astype(bf16)
    arrived = exchange(down_part.reshape(n_tp, n_near * own, rows), "tp")
    near_part = arrived.astype(f32).sum(axis=0).astype(bf16)
    arrived = exchange(near_part.reshape(n_near, own, rows), LO)
    lowered = arrived.astype(f32).sum(axis=0)
    mixed = (middle_own.astype(f32) + lowered).astype(bf16).T
    return (mixed, new_state)


def solution(mesh):
    near = min(NEIGHBOURS, mesh.shape["kv"])
    devices = mesh.devices.reshape(mesh.shape["grp"], -1, near // 2, 2, mesh.shape["tp"])
    fine = Mesh(devices, ("grp", *KV, "tp"))
    every = (*KV, "tp")
    return jax.shard_map(
        local,
        mesh=fine,
        in_specs=(
            P("grp", every),
            P(("grp", *KV), "tp", None, None),
            P(KV),
            P(KV, "tp"),
            P(KV, "tp"),
            P(KV, "tp"),
            P(),
            P(),
            P("tp"),
            P("tp"),
            P(),
            P("tp", KV),
            P(KV),
            P(KV, "tp"),
            P("tp", KV),
        ),
        out_specs=(P("grp", every), P(("grp", *KV), "tp", None, None)),
        check_vma=False,
    )
```

```python
import jax
import jax.numpy as jnp
from jax import lax
from jax.sharding import Mesh
from jax.sharding import PartitionSpec as P


epsilon = 1e-06
bf16 = jnp.bfloat16
f32 = jnp.float32
KV = ("hi", "mid", "pair")
LO = ("mid", "pair")
NEAR = (*LO, "tp")
NEIGHBOURS = 4


def exchange(x, axis):
    return lax.all_to_all(x, axis, split_axis=0, concat_axis=0, tiled=True)


def from_everyone(x, axis):
    return exchange(jnp.broadcast_to(x, (lax.axis_size(axis), *x.shape)), axis)


def dotted(left, right, left_dim, right_dim):
    dims = (((left_dim,), (right_dim,)), ((), ()))
    return lax.dot_general(left, right, dims, preferred_element_type=f32)


def delta_update(
    query_pre, key_pre, value_pre, beta_pre, decay_pre, state, a_log, dt_bias, head_gain
):
    query = query_pre * lax.rsqrt(jnp.sum(query_pre * query_pre, axis=-1, keepdims=True) + epsilon)
    keyed = key_pre * lax.rsqrt(jnp.sum(key_pre * key_pre, axis=-1, keepdims=True) + epsilon)
    beta = jax.nn.sigmoid(beta_pre)
    decay = jnp.exp(-jnp.exp(a_log) * jax.nn.softplus(decay_pre + dt_bias))
    key_read = jnp.einsum("bhk,bhkv->bhv", keyed, state)
    query_read = jnp.einsum("bhk,bhkv->bhv", query, state)
    fresh = beta[..., None] * (value_pre - decay[..., None] * key_read)
    new_state = decay[..., None, None] * state + keyed[..., :, None] * fresh[..., None, :]
    intersection = jnp.sum(query * keyed, axis=-1)
    reading = decay[..., None] * query_read + intersection[..., None] * fresh
    normed = (
        reading
        * lax.rsqrt(jnp.mean(reading * reading, axis=-1, keepdims=True) + epsilon)
        * head_gain
    )
    return (normed.astype(bf16), new_state)


def mixer_weights(w_up, w_down, mixer_gain):
    near = lax.axis_size(LO)
    me = lax.axis_index(LO)
    block, wide = w_up.shape
    share = wide // near
    gained = (w_up.astype(f32) * mixer_gain.astype(f32)[:, None]).astype(bf16)
    both = jnp.concatenate([gained, w_down.T], axis=0)
    both = both.reshape(2 * block, near, share).transpose(1, 0, 2)
    whole = jnp.zeros_like(both)
    for step in range(near):
        piece = lax.dynamic_slice_in_dim(both, me ^ step, 1, axis=0)
        if step:
            piece = lax.ppermute(piece, LO, [(i, i ^ step) for i in range(near)])
        whole = lax.dynamic_update_slice_in_dim(whole, piece, me ^ step, axis=0)
    up = whole[:, :block].reshape(near * block, share)
    down_t = whole[:, block:].reshape(near * block, share)
    return up, down_t


def local(
    tokens,
    state,
    norm_gain,
    w_query,
    w_key,
    w_value,
    w_beta,
    w_decay,
    a_log,
    dt_bias,
    head_gain,
    w_out,
    mixer_gain,
    w_up,
    w_down,
):
    seq_here, heads_here, head_size = state.shape[:3]
    n_kv = lax.axis_size(KV)
    n_tp = lax.axis_size("tp")
    n_near = lax.axis_size(LO)
    width = w_beta.shape[0]
    rows, own = tokens.shape
    block = own * n_tp
    kv_index = lax.axis_index(KV)
    tp_index = lax.axis_index("tp")
    side = lax.axis_index("pair")
    columns = heads_here * head_size
    assert heads_here == lax.axis_size("pair")

    tokens_t = tokens.T
    gain = norm_gain.astype(f32)[:, None]
    split = lambda w: w.reshape(block, heads_here, head_size).transpose(1, 0, 2)
    by_head = jnp.concatenate([split(w_query), split(w_key), split(w_value)], axis=2)
    by_head = (by_head.astype(f32) * gain).astype(bf16)
    kept = lax.dynamic_index_in_dim(by_head, side, 0, keepdims=False)
    given = lax.dynamic_index_in_dim(by_head, 1 - side, 0, keepdims=False)
    taken = lax.ppermute(given, "pair", [(0, 1), (1, 0)])

    both = from_everyone(tokens_t, ("pair", "tp")).reshape(2, block, rows)
    mine = lax.dynamic_index_in_dim(both, side, 0, keepdims=False)
    other = lax.dynamic_index_in_dim(both, 1 - side, 0, keepdims=False)
    inputs = mine.astype(f32)
    scaled = (inputs * gain).astype(bf16)
    squares = jnp.sum(inputs * inputs, axis=0)
    at = (kv_index * block, tp_index * heads_here)
    beta_rows = lax.dynamic_slice(w_beta, at, (block, heads_here))
    decay_rows = lax.dynamic_slice(w_decay, at, (block, heads_here))
    parts = [
        (dotted(mine, kept, 0, 0) + dotted(other, taken, 0, 0)).astype(bf16),
        dotted(scaled, jnp.concatenate([beta_rows, decay_rows], axis=1), 0, 0).astype(bf16),
        squares[:, None].astype(bf16),
    ]
    sent = jnp.concatenate(parts, axis=1).reshape(n_kv, seq_here, -1)
    arrived = exchange(sent, KV)
    main = 3 * head_size
    sums = arrived.astype(f32)
    gates = sums[..., main:].sum(axis=0)
    sums = sums[..., :main].reshape(-1, heads_here, seq_here, main).sum(axis=0)
    first = lax.rsqrt(gates[:, -1:] / width + epsilon)
    pre = (first * sums).transpose(1, 0, 2)
    gates = first * gates
    heads = lambda n: pre[..., n * head_size : (n + 1) * head_size]
    normed, new_state = delta_update(
        heads(0),
        heads(1),
        heads(2),
        gates[:, :heads_here],
        gates[:, heads_here : 2 * heads_here],
        state,
        a_log,
        dt_bias,
        head_gain,
    )
    up, down_t = mixer_weights(w_up, w_down, mixer_gain)

    every = from_everyone(normed.reshape(seq_here, columns), KV).reshape(rows, columns)
    head_part = dotted(w_out, every, 0, 1).astype(bf16)
    attended = from_everyone(head_part, "tp").astype(f32).sum(axis=0)
    middle_block = (inputs + attended).astype(bf16)
    middle_own = lax.dynamic_slice_in_dim(middle_block, tp_index * own, own, axis=0)

    middle = from_everyone(middle_block, LO).reshape(n_near * block, rows)
    middle_f = middle.astype(f32)
    squares_two = jnp.sum(middle_f * middle_f, axis=0, keepdims=True)
    hidden_part = dotted(up, middle, 0, 0)
    far = lax.axis_size("hi")
    hidden_part = hidden_part.reshape(far, -1, rows)
    tail = jnp.broadcast_to(squares_two, (far, 8, rows))
    sent = jnp.concatenate([hidden_part, tail], axis=1).astype(bf16)
    sums = exchange(sent, "hi").astype(f32).sum(axis=0)
    second = lax.rsqrt(sums[-1:] / width + epsilon)
    hidden_own = jnp.square(jax.nn.relu(second * sums[:-8])).astype(bf16)
    hidden = from_everyone(hidden_own, "hi").reshape(-1, rows)
    down_part = dotted(down_t, hidden, 1, 0).astype(bf16)
    arrived = exchange(down_part.reshape(n_near * n_tp, own, rows), NEAR)
    lowered = arrived.astype(f32).sum(axis=0)
    mixed = (middle_own.astype(f32) + lowered).astype(bf16).T
    return (mixed, new_state)


def solution(mesh):
    near = min(NEIGHBOURS, mesh.shape["kv"])
    devices = mesh.devices.reshape(mesh.shape["grp"], -1, near // 2, 2, mesh.shape["tp"])
    fine = Mesh(devices, ("grp", *KV, "tp"))
    every = (*KV, "tp")
    return jax.shard_map(
        local,
        mesh=fine,
        in_specs=(
            P("grp", every),
            P(("grp", *KV), "tp", None, None),
            P(KV),
            P(KV, "tp"),
            P(KV, "tp"),
            P(KV, "tp"),
            P(),
            P(),
            P("tp"),
            P("tp"),
            P(),
            P("tp", KV),
            P(KV),
            P(KV, "tp"),
            P("tp", KV),
        ),
        out_specs=(P("grp", every), P(("grp", *KV), "tp", None, None)),
        check_vma=False,
    )
```

```python
import jax
import jax.numpy as jnp
from jax import lax
from jax.sharding import Mesh
from jax.sharding import PartitionSpec as P


epsilon = 1e-06
bf16 = jnp.bfloat16
f32 = jnp.float32
KV = ("hi", "mid", "pair")
LO = ("mid", "pair")
NEAR = (*LO, "tp")
NEIGHBOURS = 4


def exchange(x, axis):
    return lax.all_to_all(x, axis, split_axis=0, concat_axis=0, tiled=True)


def from_everyone(x, axis):
    return exchange(jnp.broadcast_to(x, (lax.axis_size(axis), *x.shape)), axis)


def dotted(left, right, left_dim, right_dim):
    dims = (((left_dim,), (right_dim,)), ((), ()))
    return lax.dot_general(left, right, dims, preferred_element_type=f32)


def delta_update(
    query_pre, key_pre, value_pre, beta_pre, decay_pre, state, a_log, dt_bias, head_gain
):
    query = query_pre * lax.rsqrt(jnp.sum(query_pre * query_pre, axis=-1, keepdims=True) + epsilon)
    keyed = key_pre * lax.rsqrt(jnp.sum(key_pre * key_pre, axis=-1, keepdims=True) + epsilon)
    beta = jax.nn.sigmoid(beta_pre)
    decay = jnp.exp(-jnp.exp(a_log) * jax.nn.softplus(decay_pre + dt_bias))
    key_read = jnp.einsum("bhk,bhkv->bhv", keyed, state)
    query_read = jnp.einsum("bhk,bhkv->bhv", query, state)
    fresh = beta[..., None] * (value_pre - decay[..., None] * key_read)
    new_state = decay[..., None, None] * state + keyed[..., :, None] * fresh[..., None, :]
    intersection = jnp.sum(query * keyed, axis=-1)
    reading = decay[..., None] * query_read + intersection[..., None] * fresh
    normed = (
        reading
        * lax.rsqrt(jnp.mean(reading * reading, axis=-1, keepdims=True) + epsilon)
        * head_gain
    )
    return (normed.astype(bf16), new_state)


def mixer_pieces(w_up, w_down, mixer_gain):
    near = lax.axis_size(LO)
    me = lax.axis_index(LO)
    block, wide = w_up.shape
    gained = (w_up.astype(f32) * mixer_gain.astype(f32)[:, None]).astype(bf16)
    both = jnp.concatenate([gained, w_down.T], axis=0)
    both = both.reshape(2 * block, near, wide // near).transpose(1, 0, 2)
    return [lax.dynamic_index_in_dim(both, me ^ step, 0, keepdims=False) for step in range(near)]


def mixer_weights(pieces):
    near = lax.axis_size(LO)
    me = lax.axis_index(LO)
    both, share = pieces[0].shape
    whole = jnp.zeros((near, both, share), bf16)
    for step, piece in enumerate(pieces):
        if step:
            piece = lax.ppermute(piece, LO, [(i, i ^ step) for i in range(near)])
        whole = lax.dynamic_update_slice_in_dim(whole, piece[None], me ^ step, axis=0)
    block = both // 2
    up = whole[:, :block].reshape(near * block, share)
    down_t = whole[:, block:].reshape(near * block, share)
    return up, down_t


def local(
    tokens,
    state,
    norm_gain,
    w_query,
    w_key,
    w_value,
    w_beta,
    w_decay,
    a_log,
    dt_bias,
    head_gain,
    w_out,
    mixer_gain,
    w_up,
    w_down,
):
    seq_here, heads_here, head_size = state.shape[:3]
    n_kv = lax.axis_size(KV)
    n_tp = lax.axis_size("tp")
    n_near = lax.axis_size(LO)
    width = w_beta.shape[0]
    rows, own = tokens.shape
    block = own * n_tp
    kv_index = lax.axis_index(KV)
    tp_index = lax.axis_index("tp")
    side = lax.axis_index("pair")
    columns = heads_here * head_size
    assert heads_here == lax.axis_size("pair")

    tokens_t = tokens.T
    gain = norm_gain.astype(f32)[:, None]
    split = lambda w: w.reshape(block, heads_here, head_size).transpose(1, 0, 2)
    by_head = jnp.concatenate([split(w_query), split(w_key), split(w_value)], axis=2)
    by_head = (by_head.astype(f32) * gain).astype(bf16)
    kept = lax.dynamic_index_in_dim(by_head, side, 0, keepdims=False)
    given = lax.dynamic_index_in_dim(by_head, 1 - side, 0, keepdims=False)
    taken = lax.ppermute(given, "pair", [(0, 1), (1, 0)])

    both = from_everyone(tokens_t, ("pair", "tp")).reshape(2, block, rows)
    mine = lax.dynamic_index_in_dim(both, side, 0, keepdims=False)
    other = lax.dynamic_index_in_dim(both, 1 - side, 0, keepdims=False)
    inputs = mine.astype(f32)
    scaled = (inputs * gain).astype(bf16)
    squares = jnp.sum(inputs * inputs, axis=0)
    at = (kv_index * block, tp_index * heads_here)
    beta_rows = lax.dynamic_slice(w_beta, at, (block, heads_here))
    decay_rows = lax.dynamic_slice(w_decay, at, (block, heads_here))
    parts = [
        (dotted(mine, kept, 0, 0) + dotted(other, taken, 0, 0)).astype(bf16),
        dotted(scaled, jnp.concatenate([beta_rows, decay_rows], axis=1), 0, 0).astype(bf16),
        squares[:, None].astype(bf16),
    ]
    sent = jnp.concatenate(parts, axis=1).reshape(n_kv, seq_here, -1)
    pieces = mixer_pieces(w_up, w_down, mixer_gain)
    arrived = exchange(sent, KV)
    arrived, *pieces = lax.optimization_barrier((arrived, *pieces))
    main = 3 * head_size
    sums = arrived.astype(f32)
    gates = sums[..., main:].sum(axis=0)
    sums = sums[..., :main].reshape(-1, heads_here, seq_here, main).sum(axis=0)
    first = lax.rsqrt(gates[:, -1:] / width + epsilon)
    pre = (first * sums).transpose(1, 0, 2)
    gates = first * gates
    heads = lambda n: pre[..., n * head_size : (n + 1) * head_size]
    normed, new_state = delta_update(
        heads(0),
        heads(1),
        heads(2),
        gates[:, :heads_here],
        gates[:, heads_here : 2 * heads_here],
        state,
        a_log,
        dt_bias,
        head_gain,
    )
    up, down_t = mixer_weights(pieces)

    every = from_everyone(normed.reshape(seq_here, columns), KV).reshape(rows, columns)
    head_part = dotted(w_out, every, 0, 1).astype(bf16)
    attended = from_everyone(head_part, "tp").astype(f32).sum(axis=0)
    middle_block = (inputs + attended).astype(bf16)
    middle_own = lax.dynamic_slice_in_dim(middle_block, tp_index * own, own, axis=0)

    middle = from_everyone(middle_block, LO).reshape(n_near * block, rows)
    middle_f = middle.astype(f32)
    squares_two = jnp.sum(middle_f * middle_f, axis=0, keepdims=True)
    hidden_part = dotted(up, middle, 0, 0)
    far = lax.axis_size("hi")
    hidden_part = hidden_part.reshape(far, -1, rows)
    tail = jnp.broadcast_to(squares_two, (far, 8, rows))
    sent = jnp.concatenate([hidden_part, tail], axis=1).astype(bf16)
    sums = exchange(sent, "hi").astype(f32).sum(axis=0)
    second = lax.rsqrt(sums[-1:] / width + epsilon)
    hidden_own = jnp.square(jax.nn.relu(second * sums[:-8])).astype(bf16)
    hidden = from_everyone(hidden_own, "hi").reshape(-1, rows)
    down_part = dotted(down_t, hidden, 1, 0).astype(bf16)
    arrived = exchange(down_part.reshape(n_near * n_tp, own, rows), NEAR)
    lowered = arrived.astype(f32).sum(axis=0)
    mixed = (middle_own.astype(f32) + lowered).astype(bf16).T
    return (mixed, new_state)


def solution(mesh):
    near = min(NEIGHBOURS, mesh.shape["kv"])
    devices = mesh.devices.reshape(mesh.shape["grp"], -1, near // 2, 2, mesh.shape["tp"])
    fine = Mesh(devices, ("grp", *KV, "tp"))
    every = (*KV, "tp")
    return jax.shard_map(
        local,
        mesh=fine,
        in_specs=(
            P("grp", every),
            P(("grp", *KV), "tp", None, None),
            P(KV),
            P(KV, "tp"),
            P(KV, "tp"),
            P(KV, "tp"),
            P(),
            P(),
            P("tp"),
            P("tp"),
            P(),
            P("tp", KV),
            P(KV),
            P(KV, "tp"),
            P("tp", KV),
        ),
        out_specs=(P("grp", every), P(("grp", *KV), "tp", None, None)),
        check_vma=False,
    )
```

```python
import functools

import jax
import jax.numpy as jnp
from jax import lax
from jax.experimental import pallas as pl
from jax.experimental.pallas import tpu as pltpu
from jax.sharding import Mesh
from jax.sharding import PartitionSpec as P


epsilon = 1e-06
bf16 = jnp.bfloat16
f32 = jnp.float32
KV = ("hi", "mid", "pair")
LO = ("mid", "pair")
NEAR = (*LO, "tp")
NEIGHBOURS = 4


def exchange(x, axis):
    return lax.all_to_all(x, axis, split_axis=0, concat_axis=0, tiled=True)


def from_everyone(x, axis):
    return exchange(jnp.broadcast_to(x, (lax.axis_size(axis), *x.shape)), axis)


def dotted(left, right, left_dim, right_dim):
    dims = (((left_dim,), (right_dim,)), ((), ()))
    return lax.dot_general(left, right, dims, preferred_element_type=f32)


def delta_kernel(arrived, state, a_log, dt_bias, head_gain, normed_all, keyed_out, fresh_out, decay_out, *, width):
    n_kv, seq, _ = arrived.shape
    heads = state.shape[1]
    size = state.shape[3]
    main = 3 * size
    sums = []
    for head in range(heads):
        total = arrived[head].astype(f32)
        for source in range(head + heads, n_kv, heads):
            total = total + arrived[source].astype(f32)
        sums.append(total)
    gates = sums[0][:, main:]
    for total in sums[1:]:
        gates = gates + total[:, main:]
    first = lax.rsqrt(gates[:, 2 * heads : 2 * heads + 1] / width + epsilon)
    normed = []
    for head in range(heads):
        pre = first * sums[head][:, :main]
        query, key, value = (pre[:, n * size : (n + 1) * size] for n in range(3))
        query = query * lax.rsqrt(jnp.sum(query * query, axis=1, keepdims=True) + epsilon)
        key = key * lax.rsqrt(jnp.sum(key * key, axis=1, keepdims=True) + epsilon)
        beta = jax.nn.sigmoid(first * gates[:, head : head + 1])
        logit = first * gates[:, heads + head : heads + head + 1] + dt_bias[:, head : head + 1]
        soft = jnp.maximum(logit, 0.0) + jnp.log1p(jnp.exp(-jnp.abs(logit)))
        decay = jnp.exp(-jnp.exp(a_log[:, head : head + 1]) * soft)
        turned = jnp.transpose(jnp.concatenate([query, key], axis=0))
        reads = []
        for row in range(seq):
            matrix = state[row, head]
            reads.append(
                (
                    jnp.sum(matrix * turned[:, row : row + 1], axis=0, keepdims=True),
                    jnp.sum(matrix * turned[:, seq + row : seq + row + 1], axis=0, keepdims=True),
                )
            )
        query_read = jnp.concatenate([r[0] for r in reads], axis=0)
        key_read = jnp.concatenate([r[1] for r in reads], axis=0)
        fresh = beta * (value - decay * key_read)
        both = jnp.sum(query * key, axis=1, keepdims=True)
        reading = decay * query_read + both * fresh
        square = jnp.sum(reading * reading, axis=1, keepdims=True) / size
        normed.append(reading * lax.rsqrt(square + epsilon) * head_gain[...])
        keyed_out[head] = key
        fresh_out[head] = fresh
        decay_out[head] = jnp.broadcast_to(decay, (seq, size))
    whole = jnp.concatenate(normed, axis=1).astype(bf16)
    for target in range(n_kv):
        normed_all[target] = whole


def state_kernel(state, keyed, fresh, decay, new_state):
    seq, heads, _, _ = state.shape
    for head in range(heads):
        turned = jnp.transpose(jnp.concatenate([keyed[head], decay[head]], axis=0))
        for row in range(seq):
            column = turned[:, row : row + 1]
            scale = turned[:, seq + row : seq + row + 1]
            new_state[row, head] = scale * state[row, head] + column * fresh[head, row : row + 1, :]


def delta_update(arrived, state, a_log, dt_bias, head_gain, width):
    n_kv, seq, _ = arrived.shape
    heads, size = state.shape[1:3]
    small = pltpu.VMEM((heads, seq, size), f32)
    arrived = pltpu.with_memory_space_constraint(arrived, pltpu.VMEM)
    state = pltpu.with_memory_space_constraint(state, pltpu.VMEM)
    return pl.pallas_call(
        functools.partial(delta_kernel, width=width),
        out_shape=(pltpu.VMEM((n_kv, seq, heads * size), bf16), small, small, small),
    )(arrived, state, a_log[None], dt_bias[None], head_gain[None])


def state_update(state, keyed, fresh, decay):
    small = [pltpu.with_memory_space_constraint(x, pltpu.VMEM) for x in (keyed, fresh, decay)]
    return pl.pallas_call(state_kernel, out_shape=jax.ShapeDtypeStruct(state.shape, f32))(state, *small)


def mixer_weights(w_up, w_down, mixer_gain):
    near = lax.axis_size(LO)
    me = lax.axis_index(LO)
    block, wide = w_up.shape
    share = wide // near
    gained = (w_up.astype(f32) * mixer_gain.astype(f32)[:, None]).astype(bf16)
    both = jnp.concatenate([gained, w_down.T], axis=0)
    both = both.reshape(2 * block, near, share).transpose(1, 0, 2)
    whole = jnp.zeros_like(both)
    for step in range(near):
        piece = lax.dynamic_slice_in_dim(both, me ^ step, 1, axis=0)
        if step:
            piece = lax.ppermute(piece, LO, [(i, i ^ step) for i in range(near)])
        whole = lax.dynamic_update_slice_in_dim(whole, piece, me ^ step, axis=0)
    up = whole[:, :block].reshape(near * block, share)
    down_t = whole[:, block:].reshape(near * block, share)
    return up, down_t


def local(
    tokens,
    state,
    norm_gain,
    w_query,
    w_key,
    w_value,
    w_beta,
    w_decay,
    a_log,
    dt_bias,
    head_gain,
    w_out,
    mixer_gain,
    w_up,
    w_down,
):
    seq_here, heads_here, head_size = state.shape[:3]
    n_kv = lax.axis_size(KV)
    n_tp = lax.axis_size("tp")
    n_near = lax.axis_size(LO)
    width = w_beta.shape[0]
    rows, own = tokens.shape
    block = own * n_tp
    kv_index = lax.axis_index(KV)
    tp_index = lax.axis_index("tp")
    side = lax.axis_index("pair")
    columns = heads_here * head_size
    assert heads_here == lax.axis_size("pair")

    tokens_t = tokens.T
    gain = norm_gain.astype(f32)[:, None]
    split = lambda w: w.reshape(block, heads_here, head_size).transpose(1, 0, 2)
    by_head = jnp.concatenate([split(w_query), split(w_key), split(w_value)], axis=2)
    by_head = (by_head.astype(f32) * gain).astype(bf16)
    kept = lax.dynamic_index_in_dim(by_head, side, 0, keepdims=False)
    given = lax.dynamic_index_in_dim(by_head, 1 - side, 0, keepdims=False)
    taken = lax.ppermute(given, "pair", [(0, 1), (1, 0)])

    both = from_everyone(tokens_t, ("pair", "tp")).reshape(2, block, rows)
    mine = lax.dynamic_index_in_dim(both, side, 0, keepdims=False)
    other = lax.dynamic_index_in_dim(both, 1 - side, 0, keepdims=False)
    inputs = mine.astype(f32)
    scaled = (inputs * gain).astype(bf16)
    squares = jnp.sum(inputs * inputs, axis=0)
    at = (kv_index * block, tp_index * heads_here)
    beta_rows = lax.dynamic_slice(w_beta, at, (block, heads_here))
    decay_rows = lax.dynamic_slice(w_decay, at, (block, heads_here))
    parts = [
        (dotted(mine, kept, 0, 0) + dotted(other, taken, 0, 0)).astype(bf16),
        dotted(scaled, jnp.concatenate([beta_rows, decay_rows], axis=1), 0, 0).astype(bf16),
        squares[:, None].astype(bf16),
    ]
    sent = jnp.concatenate(parts, axis=1).reshape(n_kv, seq_here, -1)
    arrived = exchange(sent, KV)
    up, down_t = mixer_weights(w_up, w_down, mixer_gain)
    normed_all, keyed, fresh, decay = delta_update(arrived, state, a_log, dt_bias, head_gain, width)
    every = exchange(normed_all, KV).reshape(rows, columns)
    new_state = state_update(state, keyed, fresh, decay)
    head_part = dotted(w_out, every, 0, 1).astype(bf16)
    attended = from_everyone(head_part, "tp").astype(f32).sum(axis=0)
    middle_block = (inputs + attended).astype(bf16)
    middle_own = lax.dynamic_slice_in_dim(middle_block, tp_index * own, own, axis=0)

    middle = from_everyone(middle_block, LO).reshape(n_near * block, rows)
    middle_f = middle.astype(f32)
    squares_two = jnp.sum(middle_f * middle_f, axis=0, keepdims=True)
    hidden_part = dotted(up, middle, 0, 0)
    far = lax.axis_size("hi")
    hidden_part = hidden_part.reshape(far, -1, rows)
    tail = jnp.broadcast_to(squares_two, (far, 8, rows))
    sent = jnp.concatenate([hidden_part, tail], axis=1).astype(bf16)
    sums = exchange(sent, "hi").astype(f32).sum(axis=0)
    second = lax.rsqrt(sums[-1:] / width + epsilon)
    hidden_own = jnp.square(jax.nn.relu(second * sums[:-8])).astype(bf16)
    hidden = from_everyone(hidden_own, "hi").reshape(-1, rows)
    down_part = dotted(down_t, hidden, 1, 0).astype(bf16)
    arrived = exchange(down_part.reshape(n_near * n_tp, own, rows), NEAR)
    lowered = arrived.astype(f32).sum(axis=0)
    mixed = (middle_own.astype(f32) + lowered).astype(bf16).T
    return (mixed, new_state)


def solution(mesh):
    near = min(NEIGHBOURS, mesh.shape["kv"])
    devices = mesh.devices.reshape(mesh.shape["grp"], -1, near // 2, 2, mesh.shape["tp"])
    fine = Mesh(devices, ("grp", *KV, "tp"))
    every = (*KV, "tp")
    return jax.shard_map(
        local,
        mesh=fine,
        in_specs=(
            P("grp", every),
            P(("grp", *KV), "tp", None, None),
            P(KV),
            P(KV, "tp"),
            P(KV, "tp"),
            P(KV, "tp"),
            P(),
            P(),
            P("tp"),
            P("tp"),
            P(),
            P("tp", KV),
            P(KV),
            P(KV, "tp"),
            P("tp", KV),
        ),
        out_specs=(P("grp", every), P(("grp", *KV), "tp", None, None)),
        check_vma=False,
    )
```

```python
import functools

import jax
import jax.numpy as jnp
from jax import lax
from jax.experimental import pallas as pl
from jax.experimental.pallas import tpu as pltpu
from jax.sharding import Mesh
from jax.sharding import PartitionSpec as P


epsilon = 1e-06
bf16 = jnp.bfloat16
f32 = jnp.float32
KV = ("hi", "mid", "pair")
LO = ("mid", "pair")
NEAR = (*LO, "tp")
NEIGHBOURS = 4


def exchange(x, axis):
    return lax.all_to_all(x, axis, split_axis=0, concat_axis=0, tiled=True)


def from_everyone(x, axis):
    return exchange(jnp.broadcast_to(x, (lax.axis_size(axis), *x.shape)), axis)


def dotted(left, right, left_dim, right_dim):
    dims = (((left_dim,), (right_dim,)), ((), ()))
    return lax.dot_general(left, right, dims, preferred_element_type=f32)


def delta_kernel(arrived, state, a_log, dt_bias, head_gain, normed_all, keyed_out, fresh_out, decay_out, *, width, all_heads):
    n_kv, seq, _ = arrived.shape
    heads = state.shape[1]
    size = state.shape[3]
    main = 3 * size
    sums = []
    for head in range(heads):
        total = arrived[head].astype(f32)
        for source in range(head + heads, n_kv, heads):
            total = total + arrived[source].astype(f32)
        sums.append(total)
    gates = sums[0][:, main:]
    for total in sums[1:]:
        gates = gates + total[:, main:]
    tp_index = lax.axis_index("tp")
    lane = lax.broadcasted_iota(jnp.int32, gates.shape, 1)
    at = lambda n: jnp.sum(jnp.where(lane == n, gates, 0.0), axis=1, keepdims=True)
    first = lax.rsqrt(at(2 * all_heads) / width + epsilon)
    normed = []
    for head in range(heads):
        pre = first * sums[head][:, :main]
        query, key, value = (pre[:, n * size : (n + 1) * size] for n in range(3))
        query = query * lax.rsqrt(jnp.sum(query * query, axis=1, keepdims=True) + epsilon)
        key = key * lax.rsqrt(jnp.sum(key * key, axis=1, keepdims=True) + epsilon)
        beta = jax.nn.sigmoid(first * at(heads * tp_index + head))
        logit = first * at(all_heads + heads * tp_index + head) + dt_bias[:, head : head + 1]
        soft = jnp.maximum(logit, 0.0) + jnp.log1p(jnp.exp(-jnp.abs(logit)))
        decay = jnp.exp(-jnp.exp(a_log[:, head : head + 1]) * soft)
        turned = jnp.transpose(jnp.concatenate([query, key], axis=0))
        reads = []
        for row in range(seq):
            matrix = state[row, head]
            reads.append(
                (
                    jnp.sum(matrix * turned[:, row : row + 1], axis=0, keepdims=True),
                    jnp.sum(matrix * turned[:, seq + row : seq + row + 1], axis=0, keepdims=True),
                )
            )
        query_read = jnp.concatenate([r[0] for r in reads], axis=0)
        key_read = jnp.concatenate([r[1] for r in reads], axis=0)
        fresh = beta * (value - decay * key_read)
        both = jnp.sum(query * key, axis=1, keepdims=True)
        reading = decay * query_read + both * fresh
        square = jnp.sum(reading * reading, axis=1, keepdims=True) / size
        normed.append(reading * lax.rsqrt(square + epsilon) * head_gain[...])
        keyed_out[head] = key
        fresh_out[head] = fresh
        decay_out[head] = jnp.broadcast_to(decay, (seq, size))
    whole = jnp.concatenate(normed, axis=1).astype(bf16)
    for target in range(n_kv):
        normed_all[target] = whole


def state_kernel(state, keyed, fresh, decay, new_state):
    seq, heads, _, _ = state.shape
    for head in range(heads):
        turned = jnp.transpose(jnp.concatenate([keyed[head], decay[head]], axis=0))
        for row in range(seq):
            column = turned[:, row : row + 1]
            scale = turned[:, seq + row : seq + row + 1]
            new_state[row, head] = scale * state[row, head] + column * fresh[head, row : row + 1, :]


def delta_update(arrived, state, a_log, dt_bias, head_gain, width, all_heads):
    n_kv, seq, _ = arrived.shape
    heads, size = state.shape[1:3]
    small = pltpu.VMEM((heads, seq, size), f32)
    arrived = pltpu.with_memory_space_constraint(arrived, pltpu.VMEM)
    state = pltpu.with_memory_space_constraint(state, pltpu.VMEM)
    whole = pl.BlockSpec(memory_space=pltpu.VMEM)
    return pl.pallas_call(
        functools.partial(delta_kernel, width=width, all_heads=all_heads),
        in_specs=[whole] * 5,
        out_shape=(pltpu.VMEM((n_kv, seq, heads * size), bf16), small, small, small),
    )(arrived, state, a_log[None], dt_bias[None], head_gain[None])


def weights_kernel(*refs):
    sources, kept, given, gates, held, arrivals = refs[:6], refs[6], refs[7], refs[8], refs[9:15], refs[15]
    block = kept.shape[0]
    size = kept.shape[1] // 3
    side = lax.axis_index("pair")
    start = pl.multiple_of(lax.axis_index(KV[:2]) * (2 * block), 2 * block)
    copies = []
    for n, (source, target) in enumerate(zip(sources, held)):
        source = source.at[:, pl.ds(start, 2 * block)] if n >= 4 else source
        copies.append(pltpu.make_async_copy(source, target, arrivals.at[n]))
    for copy in copies:
        copy.start()
    for copy in copies:
        copy.wait()
    query, key, value, gain, beta, decay = held
    wide = gain[...].astype(f32)
    column = jnp.transpose(jnp.broadcast_to(wide, (8, block)))[:, :1]
    heads = []
    for head in range(2):
        cut = slice(head * size, (head + 1) * size)
        heads.append([w[:, cut].astype(f32) * column for w in (query, key, value)])
    for n in range(3):
        cut = slice(n * size, (n + 1) * size)
        kept[:, cut] = jnp.where(side == 0, heads[0][n], heads[1][n]).astype(bf16)
        given[:, cut] = jnp.where(side == 0, heads[1][n], heads[0][n]).astype(bf16)
    both = jnp.concatenate([beta[...].astype(f32), decay[...].astype(f32)], axis=0)
    both = jnp.where(side == 0, both[:, :block], both[:, block:])
    gates[...] = jnp.transpose(both * wide).astype(bf16)


def projection_weights(w_query, w_key, w_value, norm_gain, w_beta, w_decay, size):
    block = w_query.shape[0]
    assert 2 * block % 128 == 0
    sources = (w_query, w_key, w_value, norm_gain[None], w_beta.T, w_decay.T)
    held = [pltpu.VMEM(x.shape, bf16) for x in sources[:4]]
    held += [pltpu.VMEM((x.shape[0], 2 * block), bf16) for x in sources[4:]]
    cut = pltpu.VMEM((block, 3 * size), bf16)
    return pl.pallas_call(
        weights_kernel,
        in_specs=[pl.BlockSpec(memory_space=pl.ANY)] * 6,
        out_shape=(cut, cut, pltpu.VMEM((block, 2 * w_beta.shape[1]), bf16)),
        scratch_shapes=[*held, pltpu.SemaphoreType.DMA((6,))],
    )(*sources)


def sums_kernel(both, kept, taken, gates, sent):
    n_kv, seq, columns = sent.shape
    side = lax.axis_index("pair")
    mine = jnp.transpose(both[side].astype(f32))
    other = jnp.transpose(both[1 - side].astype(f32))
    squares = jnp.sum(mine * mine, axis=1, keepdims=True)
    mine = mine.astype(bf16)
    main = dotted(mine, kept[...], 1, 0) + dotted(other.astype(bf16), taken[...], 1, 0)
    extra = dotted(mine, gates[...], 1, 0)
    spare = columns - main.shape[1] - extra.shape[1] - 1
    tail = jnp.concatenate([extra, squares, jnp.zeros((mine.shape[0], spare), f32)], axis=1)
    whole = jnp.concatenate([main, tail], axis=1)
    for target in range(n_kv):
        sent[target] = whole[target * seq : (target + 1) * seq].astype(bf16)


def partial_sums(both, kept, taken, gates, n_kv, seq):
    whole = pl.BlockSpec(memory_space=pltpu.VMEM)
    columns = kept.shape[1] + 128
    near = [pltpu.with_memory_space_constraint(x, pltpu.VMEM) for x in (both, kept, taken, gates)]
    return pl.pallas_call(
        sums_kernel,
        in_specs=[whole] * 4,
        out_shape=jax.ShapeDtypeStruct((n_kv, seq, columns), bf16),
    )(*near)


def state_update(state, keyed, fresh, decay):
    small = [pltpu.with_memory_space_constraint(x, pltpu.VMEM) for x in (keyed, fresh, decay)]
    return pl.pallas_call(state_kernel, out_shape=jax.ShapeDtypeStruct(state.shape, f32))(state, *small)


def mixer_pieces(w_up, w_down, mixer_gain):
    near = lax.axis_size(LO)
    me = lax.axis_index(LO)
    block, wide = w_up.shape
    gained = (w_up.astype(f32) * mixer_gain.astype(f32)[:, None]).astype(bf16)
    both = jnp.concatenate([gained, w_down.T], axis=0)
    both = both.reshape(2 * block, near, wide // near).transpose(1, 0, 2)
    return [lax.dynamic_index_in_dim(both, me ^ step, 0, keepdims=False) for step in range(near)]


def mixer_weights(pieces):
    near = lax.axis_size(LO)
    me = lax.axis_index(LO)
    both, share = pieces[0].shape
    whole = jnp.zeros((near, both, share), bf16)
    for step, piece in enumerate(pieces):
        if step:
            piece = lax.ppermute(piece, LO, [(i, i ^ step) for i in range(near)])
        whole = lax.dynamic_update_slice_in_dim(whole, piece[None], me ^ step, axis=0)
    block = both // 2
    up = whole[:, :block].reshape(near * block, share)
    down_t = whole[:, block:].reshape(near * block, share)
    return up, down_t


def local(
    tokens,
    state,
    norm_gain,
    w_query,
    w_key,
    w_value,
    w_beta,
    w_decay,
    a_log,
    dt_bias,
    head_gain,
    w_out,
    mixer_gain,
    w_up,
    w_down,
):
    seq_here, heads_here, head_size = state.shape[:3]
    n_kv = lax.axis_size(KV)
    n_tp = lax.axis_size("tp")
    n_near = lax.axis_size(LO)
    width = w_beta.shape[0]
    rows, own = tokens.shape
    block = own * n_tp
    tp_index = lax.axis_index("tp")
    side = lax.axis_index("pair")
    columns = heads_here * head_size
    assert heads_here == lax.axis_size("pair")

    tokens_t = tokens.T
    kept, given, gates = projection_weights(
        w_query, w_key, w_value, norm_gain, w_beta, w_decay, head_size
    )
    taken = lax.ppermute(given, "pair", [(0, 1), (1, 0)])

    both = from_everyone(tokens_t, ("pair", "tp")).reshape(2, block, rows)
    inputs = lax.dynamic_index_in_dim(both, side, 0, keepdims=False).astype(f32)
    sent = partial_sums(both, kept, taken, gates, n_kv, seq_here)
    pieces = mixer_pieces(w_up, w_down, mixer_gain)
    arrived = exchange(sent, KV)
    up, down_t = mixer_weights(pieces)
    normed_all, keyed, fresh, decay = delta_update(arrived, state, a_log, dt_bias, head_gain, width, w_beta.shape[1])
    every = exchange(normed_all, KV).reshape(rows, columns)
    new_state = state_update(state, keyed, fresh, decay)
    head_part = dotted(w_out, every, 0, 1).astype(bf16)
    attended = from_everyone(head_part, "tp").astype(f32).sum(axis=0)
    middle_block = (inputs + attended).astype(bf16)
    middle_own = lax.dynamic_slice_in_dim(middle_block, tp_index * own, own, axis=0)

    middle = from_everyone(middle_block, LO).reshape(n_near * block, rows)
    middle_f = middle.astype(f32)
    squares_two = jnp.sum(middle_f * middle_f, axis=0, keepdims=True)
    hidden_part = dotted(up, middle, 0, 0)
    far = lax.axis_size("hi")
    hidden_part = hidden_part.reshape(far, -1, rows)
    tail = jnp.broadcast_to(squares_two, (far, 8, rows))
    sent = jnp.concatenate([hidden_part, tail], axis=1).astype(bf16)
    sums = exchange(sent, "hi").astype(f32).sum(axis=0)
    second = lax.rsqrt(sums[-1:] / width + epsilon)
    hidden_own = jnp.square(jax.nn.relu(second * sums[:-8])).astype(bf16)
    hidden = from_everyone(hidden_own, "hi").reshape(-1, rows)
    down_part = dotted(down_t, hidden, 1, 0).astype(bf16)
    arrived = exchange(down_part.reshape(n_near * n_tp, own, rows), NEAR)
    lowered = arrived.astype(f32).sum(axis=0)
    mixed = (middle_own.astype(f32) + lowered).astype(bf16).T
    return (mixed, new_state)


def solution(mesh):
    near = min(NEIGHBOURS, mesh.shape["kv"])
    devices = mesh.devices.reshape(mesh.shape["grp"], -1, near // 2, 2, mesh.shape["tp"])
    fine = Mesh(devices, ("grp", *KV, "tp"))
    every = (*KV, "tp")
    return jax.shard_map(
        local,
        mesh=fine,
        in_specs=(
            P("grp", every),
            P(("grp", *KV), "tp", None, None),
            P(KV),
            P(KV, "tp"),
            P(KV, "tp"),
            P(KV, "tp"),
            P(),
            P(),
            P("tp"),
            P("tp"),
            P(),
            P("tp", KV),
            P(KV),
            P(KV, "tp"),
            P("tp", KV),
        ),
        out_specs=(P("grp", every), P(("grp", *KV), "tp", None, None)),
        check_vma=False,
    )
```

```python
import functools

import jax
import jax.numpy as jnp
from jax import lax
from jax.experimental import pallas as pl
from jax.experimental.pallas import tpu as pltpu
from jax.sharding import Mesh
from jax.sharding import PartitionSpec as P


epsilon = 1e-06
bf16 = jnp.bfloat16
f32 = jnp.float32
KV = ("hi", "mid", "pair")
LO = ("mid", "pair")
NEAR = (*LO, "tp")
NEIGHBOURS = 4


def exchange(x, axis):
    return lax.all_to_all(x, axis, split_axis=0, concat_axis=0, tiled=True)


def from_everyone(x, axis):
    return exchange(jnp.broadcast_to(x, (lax.axis_size(axis), *x.shape)), axis)


def dotted(left, right, left_dim, right_dim):
    dims = (((left_dim,), (right_dim,)), ((), ()))
    return lax.dot_general(left, right, dims, preferred_element_type=f32)


def delta_kernel(arrived, state, a_log, dt_bias, head_gain, normed_all, keyed_out, fresh_out, decay_out, *, width, all_heads):
    n_kv, seq, _ = arrived.shape
    heads = state.shape[1]
    size = state.shape[3]
    main = 3 * size
    sums = []
    for head in range(heads):
        total = arrived[head].astype(f32)
        for source in range(head + heads, n_kv, heads):
            total = total + arrived[source].astype(f32)
        sums.append(total)
    gates = sums[0][:, main:]
    for total in sums[1:]:
        gates = gates + total[:, main:]
    tp_index = lax.axis_index("tp")
    lane = lax.broadcasted_iota(jnp.int32, gates.shape, 1)
    at = lambda n: jnp.sum(jnp.where(lane == n, gates, 0.0), axis=1, keepdims=True)
    first = lax.rsqrt(at(2 * all_heads) / width + epsilon)
    normed = []
    for head in range(heads):
        pre = first * sums[head][:, :main]
        query, key, value = (pre[:, n * size : (n + 1) * size] for n in range(3))
        query = query * lax.rsqrt(jnp.sum(query * query, axis=1, keepdims=True) + epsilon)
        key = key * lax.rsqrt(jnp.sum(key * key, axis=1, keepdims=True) + epsilon)
        beta = jax.nn.sigmoid(first * at(heads * tp_index + head))
        logit = first * at(all_heads + heads * tp_index + head) + dt_bias[:, head : head + 1]
        soft = jnp.maximum(logit, 0.0) + jnp.log1p(jnp.exp(-jnp.abs(logit)))
        decay = jnp.exp(-jnp.exp(a_log[:, head : head + 1]) * soft)
        turned = jnp.transpose(jnp.concatenate([query, key], axis=0))
        reads = []
        for row in range(seq):
            matrix = state[row, head]
            reads.append(
                (
                    jnp.sum(matrix * turned[:, row : row + 1], axis=0, keepdims=True),
                    jnp.sum(matrix * turned[:, seq + row : seq + row + 1], axis=0, keepdims=True),
                )
            )
        query_read = jnp.concatenate([r[0] for r in reads], axis=0)
        key_read = jnp.concatenate([r[1] for r in reads], axis=0)
        fresh = beta * (value - decay * key_read)
        both = jnp.sum(query * key, axis=1, keepdims=True)
        reading = decay * query_read + both * fresh
        square = jnp.sum(reading * reading, axis=1, keepdims=True) / size
        normed.append(reading * lax.rsqrt(square + epsilon) * head_gain[...])
        keyed_out[head] = key
        fresh_out[head] = fresh
        decay_out[head] = jnp.broadcast_to(decay, (seq, size))
    whole = jnp.concatenate(normed, axis=1).astype(bf16)
    for target in range(n_kv):
        normed_all[target] = whole


def state_kernel(state, keyed, fresh, decay, new_state):
    seq, heads, _, _ = state.shape
    for head in range(heads):
        turned = jnp.transpose(jnp.concatenate([keyed[head], decay[head]], axis=0))
        for row in range(seq):
            column = turned[:, row : row + 1]
            scale = turned[:, seq + row : seq + row + 1]
            new_state[row, head] = scale * state[row, head] + column * fresh[head, row : row + 1, :]


def delta_update(arrived, state, a_log, dt_bias, head_gain, width, all_heads):
    n_kv, seq, _ = arrived.shape
    heads, size = state.shape[1:3]
    small = pltpu.VMEM((heads, seq, size), f32)
    arrived = pltpu.with_memory_space_constraint(arrived, pltpu.VMEM)
    state = pltpu.with_memory_space_constraint(state, pltpu.VMEM)
    whole = pl.BlockSpec(memory_space=pltpu.VMEM)
    return pl.pallas_call(
        functools.partial(delta_kernel, width=width, all_heads=all_heads),
        in_specs=[whole] * 5,
        out_shape=(pltpu.VMEM((n_kv, seq, heads * size), bf16), small, small, small),
    )(arrived, state, a_log[None], dt_bias[None], head_gain[None])


def weights_kernel(*refs):
    sources, kept, given, gates, held, arrivals = refs[:6], refs[6], refs[7], refs[8], refs[9:15], refs[15]
    block = kept.shape[0]
    size = kept.shape[1] // 3
    side = lax.axis_index("pair")
    start = pl.multiple_of(lax.axis_index(KV[:2]) * (2 * block), 2 * block)
    copies = []
    for n, (source, target) in enumerate(zip(sources, held)):
        source = source.at[:, pl.ds(start, 2 * block)] if n >= 4 else source
        copies.append(pltpu.make_async_copy(source, target, arrivals.at[n]))
    for copy in copies:
        copy.start()
    for copy in copies:
        copy.wait()
    query, key, value, gain, beta, decay = held
    wide = gain[...].astype(f32)
    column = jnp.transpose(jnp.broadcast_to(wide, (8, block)))[:, :1]
    heads = []
    for head in range(2):
        cut = slice(head * size, (head + 1) * size)
        heads.append([w[:, cut].astype(f32) * column for w in (query, key, value)])
    for n in range(3):
        cut = slice(n * size, (n + 1) * size)
        kept[:, cut] = jnp.where(side == 0, heads[0][n], heads[1][n]).astype(bf16)
        given[:, cut] = jnp.where(side == 0, heads[1][n], heads[0][n]).astype(bf16)
    both = jnp.concatenate([beta[...].astype(f32), decay[...].astype(f32)], axis=0)
    both = jnp.where(side == 0, both[:, :block], both[:, block:])
    gates[...] = jnp.transpose(both * wide).astype(bf16)


def projection_weights(w_query, w_key, w_value, norm_gain, w_beta, w_decay, size):
    block = w_query.shape[0]
    assert 2 * block % 128 == 0
    sources = (w_query, w_key, w_value, norm_gain[None], w_beta.T, w_decay.T)
    held = [pltpu.VMEM(x.shape, bf16) for x in sources[:4]]
    held += [pltpu.VMEM((x.shape[0], 2 * block), bf16) for x in sources[4:]]
    cut = pltpu.VMEM((block, 3 * size), bf16)
    return pl.pallas_call(
        weights_kernel,
        in_specs=[pl.BlockSpec(memory_space=pl.ANY)] * 6,
        out_shape=(cut, cut, pltpu.VMEM((block, 2 * w_beta.shape[1]), bf16)),
        scratch_shapes=[*held, pltpu.SemaphoreType.DMA((6,))],
    )(*sources)


def sums_kernel(both, kept, taken, gates, sent):
    n_kv, seq, columns = sent.shape
    side = lax.axis_index("pair")
    mine = jnp.transpose(both[side].astype(f32))
    other = jnp.transpose(both[1 - side].astype(f32))
    squares = jnp.sum(mine * mine, axis=1, keepdims=True)
    mine = mine.astype(bf16)
    main = dotted(mine, kept[...], 1, 0) + dotted(other.astype(bf16), taken[...], 1, 0)
    extra = dotted(mine, gates[...], 1, 0)
    spare = columns - main.shape[1] - extra.shape[1] - 1
    tail = jnp.concatenate([extra, squares, jnp.zeros((mine.shape[0], spare), f32)], axis=1)
    whole = jnp.concatenate([main, tail], axis=1)
    for target in range(n_kv):
        sent[target] = whole[target * seq : (target + 1) * seq].astype(bf16)


def partial_sums(both, kept, taken, gates, n_kv, seq):
    whole = pl.BlockSpec(memory_space=pltpu.VMEM)
    columns = kept.shape[1] + 128
    near = [pltpu.with_memory_space_constraint(x, pltpu.VMEM) for x in (both, kept, taken, gates)]
    return pl.pallas_call(
        sums_kernel,
        in_specs=[whole] * 4,
        out_shape=jax.ShapeDtypeStruct((n_kv, seq, columns), bf16),
    )(*near)


def state_update(state, keyed, fresh, decay):
    small = [pltpu.with_memory_space_constraint(x, pltpu.VMEM) for x in (keyed, fresh, decay)]
    return pl.pallas_call(state_kernel, out_shape=jax.ShapeDtypeStruct(state.shape, f32))(state, *small)


def mixer_pieces(w_up, w_down, mixer_gain):
    near = lax.axis_size(LO)
    me = lax.axis_index(LO)
    block, wide = w_up.shape
    gained = (w_up.astype(f32) * mixer_gain.astype(f32)[:, None]).astype(bf16)
    both = jnp.concatenate([gained, w_down.T], axis=0)
    both = both.reshape(2 * block, near, wide // near).transpose(1, 0, 2)
    pieces = []
    for step in range(near):
        piece = lax.dynamic_index_in_dim(both, me ^ step, 0, keepdims=False)
        if step:
            piece = lax.ppermute(piece, LO, [(i, i ^ step) for i in range(near)])
        pieces.append(piece)
    return pieces


def in_vmem(arrays):
    return [pltpu.with_memory_space_constraint(x, pltpu.VMEM) for x in arrays]


def middle_kernel(arrived, both, sent, kept):
    own = kept.shape[0]
    side, place = lax.axis_index("pair"), lax.axis_index("tp")
    total = both[side].astype(f32)
    added = arrived[0].astype(f32)
    for source in range(1, arrived.shape[0]):
        added = added + arrived[source].astype(f32)
    block = (total + added).astype(bf16)
    for target in range(sent.shape[0]):
        sent[target] = block
    block = block.astype(f32)
    chosen = jnp.zeros(kept.shape, f32)
    for n in range(block.shape[0] // own):
        chosen = chosen + jnp.where(place == n, block[n * own : (n + 1) * own], 0.0)
    kept[...] = chosen


def middle_rows(arrived, both, near, own):
    _, block, rows = both.shape
    arrived = pltpu.with_memory_space_constraint(arrived, pltpu.VMEM)
    both = pltpu.with_memory_space_constraint(both, pltpu.VMEM)
    return pl.pallas_call(
        middle_kernel,
        out_shape=(pltpu.VMEM((near, block, rows), bf16), pltpu.VMEM((own, rows), f32)),
    )(arrived, both)


def up_kernel(middle, *refs):
    pieces, sent = refs[:-1], refs[-1]
    me = lax.axis_index(LO)
    block = middle.shape[1]
    total, squares = 0.0, 0.0
    for step, piece in enumerate(pieces):
        part = middle[me ^ step]
        weight = jnp.transpose(piece[:block].astype(f32)).astype(bf16)
        total = total + dotted(weight, part, 1, 0)
        part = part.astype(f32)
        squares = squares + jnp.sum(part * part, axis=0, keepdims=True)
    tail = jnp.broadcast_to(squares, (8, squares.shape[1])).astype(bf16)
    share = total.shape[0] // sent.shape[0]
    for target in range(sent.shape[0]):
        sent[target, :share] = total[target * share : (target + 1) * share].astype(bf16)
        sent[target, share:] = tail


def up_sums(middle, pieces, far):
    middle = pltpu.with_memory_space_constraint(middle, pltpu.VMEM)
    share = pieces[0].shape[1] // far
    shape = (far, share + 8, middle.shape[2])
    return pl.pallas_call(up_kernel, out_shape=pltpu.VMEM(shape, bf16))(middle, *in_vmem(pieces))


def down_kernel(hidden, *refs):
    pieces, sent = refs[:-1], refs[-1]
    me = lax.axis_index(LO)
    own = sent.shape[1]
    whole = jnp.concatenate([hidden[n] for n in range(hidden.shape[0])], axis=0)
    for step, piece in enumerate(pieces):
        block = piece.shape[0] // 2
        part = dotted(piece[block:], whole, 1, 0)
        for n in range(block // own):
            sent[(me ^ step) * (block // own) + n] = part[n * own : (n + 1) * own].astype(bf16)


def down_sums(hidden, pieces, own):
    hidden = pltpu.with_memory_space_constraint(hidden, pltpu.VMEM)
    slots = len(pieces) * pieces[0].shape[0] // 2 // own
    shape = jax.ShapeDtypeStruct((slots, own, hidden.shape[2]), bf16)
    return pl.pallas_call(down_kernel, out_shape=shape)(hidden, *in_vmem(pieces))


def local(
    tokens,
    state,
    norm_gain,
    w_query,
    w_key,
    w_value,
    w_beta,
    w_decay,
    a_log,
    dt_bias,
    head_gain,
    w_out,
    mixer_gain,
    w_up,
    w_down,
):
    seq_here, heads_here, head_size = state.shape[:3]
    n_kv = lax.axis_size(KV)
    n_tp = lax.axis_size("tp")
    n_near = lax.axis_size(LO)
    width = w_beta.shape[0]
    rows, own = tokens.shape
    block = own * n_tp
    columns = heads_here * head_size
    assert heads_here == lax.axis_size("pair")

    tokens_t = tokens.T
    kept, given, gates = projection_weights(
        w_query, w_key, w_value, norm_gain, w_beta, w_decay, head_size
    )
    taken = lax.ppermute(given, "pair", [(0, 1), (1, 0)])

    both = from_everyone(tokens_t, ("pair", "tp")).reshape(2, block, rows)
    sent = partial_sums(both, kept, taken, gates, n_kv, seq_here)
    pieces = mixer_pieces(w_up, w_down, mixer_gain)
    arrived = exchange(sent, KV)
    arrived, pieces[0] = lax.optimization_barrier((arrived, pieces[0]))
    normed_all, keyed, fresh, decay = delta_update(
        arrived, state, a_log, dt_bias, head_gain, width, w_beta.shape[1]
    )
    every = exchange(normed_all, KV).reshape(rows, columns)
    new_state = state_update(state, keyed, fresh, decay)
    head_part = dotted(w_out, every, 0, 1).astype(bf16)
    arrived = from_everyone(head_part, "tp")
    middle_sent, middle_own = middle_rows(arrived, both, n_near, own)
    middle_sent, *pieces = lax.optimization_barrier((middle_sent, *pieces))
    middle = exchange(middle_sent, LO)
    sent = up_sums(middle, pieces, lax.axis_size("hi"))
    sums = exchange(sent, "hi").astype(f32).sum(axis=0)
    second = lax.rsqrt(sums[-1:] / width + epsilon)
    hidden_own = jnp.square(jax.nn.relu(second * sums[:-8])).astype(bf16)
    hidden = from_everyone(hidden_own, "hi")
    sent = down_sums(hidden, pieces, own)
    lowered = exchange(sent, NEAR).astype(f32).sum(axis=0)
    mixed = (middle_own + lowered).astype(bf16).T
    return (mixed, new_state)


def solution(mesh):
    near = min(NEIGHBOURS, mesh.shape["kv"])
    devices = mesh.devices.reshape(mesh.shape["grp"], -1, near // 2, 2, mesh.shape["tp"])
    fine = Mesh(devices, ("grp", *KV, "tp"))
    every = (*KV, "tp")
    return jax.shard_map(
        local,
        mesh=fine,
        in_specs=(
            P("grp", every),
            P(("grp", *KV), "tp", None, None),
            P(KV),
            P(KV, "tp"),
            P(KV, "tp"),
            P(KV, "tp"),
            P(),
            P(),
            P("tp"),
            P("tp"),
            P(),
            P("tp", KV),
            P(KV),
            P(KV, "tp"),
            P("tp", KV),
        ),
        out_specs=(P("grp", every), P(("grp", *KV), "tp", None, None)),
        check_vma=False,
    )
```

```python
import functools

import jax
import jax.numpy as jnp
from jax import lax
from jax.experimental import pallas as pl
from jax.experimental.pallas import tpu as pltpu
from jax.sharding import Mesh
from jax.sharding import PartitionSpec as P


epsilon = 1e-06
TAIL = 64
bf16 = jnp.bfloat16
f32 = jnp.float32
KV = ("hi", "mid", "pair")
LO = ("mid", "pair")
NEAR = (*LO, "tp")
NEIGHBOURS = 4


def exchange(x, axis):
    return lax.all_to_all(x, axis, split_axis=0, concat_axis=0, tiled=True)


def from_everyone(x, axis):
    return exchange(jnp.broadcast_to(x, (lax.axis_size(axis), *x.shape)), axis)


def dotted(left, right, left_dim, right_dim):
    dims = (((left_dim,), (right_dim,)), ((), ()))
    return lax.dot_general(left, right, dims, preferred_element_type=f32)


def delta_kernel(arrived, state, a_log, dt_bias, head_gain, normed_all, keyed_out, fresh_out, decay_out, *, width, all_heads):
    n_kv = arrived.shape[0]
    seq, heads = state.shape[:2]
    size = state.shape[3]
    main = 3 * size
    sums = []
    for head in range(heads):
        total = arrived[head].astype(f32)
        for source in range(head + heads, n_kv, heads):
            total = total + arrived[source].astype(f32)
        sums.append(total)
    ends = sums[0][:, 2 * main :]
    for total in sums[1:]:
        ends = ends + total[:, 2 * main :]
    gates = jnp.concatenate([ends[:, :TAIL], ends[:, TAIL:]], axis=0)
    sums = [jnp.concatenate([x[:, :main], x[:, main : 2 * main]], axis=0) for x in sums]
    tp_index = lax.axis_index("tp")
    lane = lax.broadcasted_iota(jnp.int32, gates.shape, 1)
    at = lambda n: jnp.sum(jnp.where(lane == n, gates, 0.0), axis=1, keepdims=True)
    first = lax.rsqrt(at(2 * all_heads) / width + epsilon)
    normed = []
    for head in range(heads):
        pre = first * sums[head]
        query, key, value = (pre[:, n * size : (n + 1) * size] for n in range(3))
        query = query * lax.rsqrt(jnp.sum(query * query, axis=1, keepdims=True) + epsilon)
        key = key * lax.rsqrt(jnp.sum(key * key, axis=1, keepdims=True) + epsilon)
        beta = jax.nn.sigmoid(first * at(heads * tp_index + head))
        logit = first * at(all_heads + heads * tp_index + head) + dt_bias[:, head : head + 1]
        soft = jnp.maximum(logit, 0.0) + jnp.log1p(jnp.exp(-jnp.abs(logit)))
        decay = jnp.exp(-jnp.exp(a_log[:, head : head + 1]) * soft)
        turned = jnp.transpose(jnp.concatenate([query, key], axis=0))
        reads = []
        for row in range(seq):
            matrix = state[row, head]
            reads.append(
                (
                    jnp.sum(matrix * turned[:, row : row + 1], axis=0, keepdims=True),
                    jnp.sum(matrix * turned[:, seq + row : seq + row + 1], axis=0, keepdims=True),
                )
            )
        query_read = jnp.concatenate([r[0] for r in reads], axis=0)
        key_read = jnp.concatenate([r[1] for r in reads], axis=0)
        fresh = beta * (value - decay * key_read)
        both = jnp.sum(query * key, axis=1, keepdims=True)
        reading = decay * query_read + both * fresh
        square = jnp.sum(reading * reading, axis=1, keepdims=True) / size
        normed.append(reading * lax.rsqrt(square + epsilon) * head_gain[...])
        keyed_out[head] = key
        fresh_out[head] = fresh
        decay_out[head] = jnp.broadcast_to(decay, (seq, size))
    whole = jnp.concatenate(normed, axis=1).astype(bf16)
    for target in range(n_kv):
        normed_all[target] = whole


def state_kernel(state, keyed, fresh, decay, new_state):
    seq, heads, _, _ = state.shape
    for head in range(heads):
        turned = jnp.transpose(jnp.concatenate([keyed[head], decay[head]], axis=0))
        for row in range(seq):
            column = turned[:, row : row + 1]
            scale = turned[:, seq + row : seq + row + 1]
            new_state[row, head] = scale * state[row, head] + column * fresh[head, row : row + 1, :]


def delta_update(arrived, state, a_log, dt_bias, head_gain, width, all_heads):
    n_kv = arrived.shape[0]
    seq, heads, size = state.shape[:3]
    small = pltpu.VMEM((heads, seq, size), f32)
    arrived = pltpu.with_memory_space_constraint(arrived, pltpu.VMEM)
    state = pltpu.with_memory_space_constraint(state, pltpu.VMEM)
    whole = pl.BlockSpec(memory_space=pltpu.VMEM)
    return pl.pallas_call(
        functools.partial(delta_kernel, width=width, all_heads=all_heads),
        in_specs=[whole] * 5,
        out_shape=(pltpu.VMEM((n_kv, seq, heads * size), bf16), small, small, small),
    )(arrived, state, a_log[None], dt_bias[None], head_gain[None])


def weights_kernel(*refs):
    sources, kept, given, gates, held, arrivals = refs[:6], refs[6], refs[7], refs[8], refs[9:15], refs[15]
    block = kept.shape[0]
    size = kept.shape[1] // 3
    side = lax.axis_index("pair")
    start = pl.multiple_of(lax.axis_index(KV[:2]) * (2 * block), 2 * block)
    copies = []
    for n, (source, target) in enumerate(zip(sources, held)):
        source = source.at[:, pl.ds(start, 2 * block)] if n >= 4 else source
        copies.append(pltpu.make_async_copy(source, target, arrivals.at[n]))
    for copy in copies:
        copy.start()
    for copy in copies:
        copy.wait()
    query, key, value, gain, beta, decay = held
    wide = gain[...].astype(f32)
    column = jnp.transpose(jnp.broadcast_to(wide, (8, block)))[:, :1]
    heads = []
    for head in range(2):
        cut = slice(head * size, (head + 1) * size)
        heads.append([w[:, cut].astype(f32) * column for w in (query, key, value)])
    for n in range(3):
        cut = slice(n * size, (n + 1) * size)
        kept[:, cut] = jnp.where(side == 0, heads[0][n], heads[1][n]).astype(bf16)
        given[:, cut] = jnp.where(side == 0, heads[1][n], heads[0][n]).astype(bf16)
    both = jnp.concatenate([beta[...].astype(f32), decay[...].astype(f32)], axis=0)
    both = jnp.where(side == 0, both[:, :block], both[:, block:])
    gates[...] = jnp.transpose(both * wide).astype(bf16)


def projection_weights(w_query, w_key, w_value, norm_gain, w_beta, w_decay, size):
    block = w_query.shape[0]
    assert 2 * block % 128 == 0
    sources = (w_query, w_key, w_value, norm_gain[None], w_beta.T, w_decay.T)
    held = [pltpu.VMEM(x.shape, bf16) for x in sources[:4]]
    held += [pltpu.VMEM((x.shape[0], 2 * block), bf16) for x in sources[4:]]
    cut = pltpu.VMEM((block, 3 * size), bf16)
    return pl.pallas_call(
        weights_kernel,
        in_specs=[pl.BlockSpec(memory_space=pl.ANY)] * 6,
        out_shape=(cut, cut, pltpu.VMEM((block, 2 * w_beta.shape[1]), bf16)),
        scratch_shapes=[*held, pltpu.SemaphoreType.DMA((6,))],
    )(*sources)


def sums_kernel(both, kept, taken, gates, sent):
    n_kv, half, _ = sent.shape
    side = lax.axis_index("pair")
    mine = jnp.transpose(both[side].astype(f32))
    other = jnp.transpose(both[1 - side].astype(f32))
    squares = jnp.sum(mine * mine, axis=1, keepdims=True)
    mine = mine.astype(bf16)
    main = dotted(mine, kept[...], 1, 0) + dotted(other.astype(bf16), taken[...], 1, 0)
    extra = dotted(mine, gates[...], 1, 0)
    gap = jnp.zeros((mine.shape[0], TAIL - extra.shape[1] - 1), f32)
    tail = jnp.concatenate([extra, squares, gap], axis=1)
    blank = jnp.zeros_like(tail)
    upper = jnp.concatenate([main, tail, blank], axis=1)
    lower = jnp.concatenate([blank, tail], axis=1)
    width = main.shape[1]
    for target in range(n_kv):
        at = 2 * target * half
        top, low = slice(at, at + half), slice(at + half, at + 2 * half)
        ends = upper[top, width:] + lower[low]
        sent[target] = jnp.concatenate([upper[top, :width], main[low], ends], axis=1).astype(bf16)


def partial_sums(both, kept, taken, gates, n_kv, seq):
    whole = pl.BlockSpec(memory_space=pltpu.VMEM)
    assert seq % 2 == 0 and gates.shape[1] < TAIL
    columns = 2 * (kept.shape[1] + TAIL)
    near = [pltpu.with_memory_space_constraint(x, pltpu.VMEM) for x in (both, kept, taken, gates)]
    return pl.pallas_call(
        sums_kernel,
        in_specs=[whole] * 4,
        out_shape=jax.ShapeDtypeStruct((n_kv, seq // 2, columns), bf16),
    )(*near)


def state_update(state, keyed, fresh, decay):
    small = [pltpu.with_memory_space_constraint(x, pltpu.VMEM) for x in (keyed, fresh, decay)]
    return pl.pallas_call(state_kernel, out_shape=jax.ShapeDtypeStruct(state.shape, f32))(state, *small)


def mixer_pieces(w_up, w_down, mixer_gain):
    near = lax.axis_size(LO)
    me = lax.axis_index(LO)
    block, wide = w_up.shape
    gained = (w_up.astype(f32) * mixer_gain.astype(f32)[:, None]).astype(bf16)
    both = jnp.concatenate([gained, w_down.T], axis=0)
    both = both.reshape(2 * block, near, wide // near).transpose(1, 0, 2)
    pieces = []
    for step in range(near):
        piece = lax.dynamic_index_in_dim(both, me ^ step, 0, keepdims=False)
        if step:
            piece = lax.ppermute(piece, LO, [(i, i ^ step) for i in range(near)])
        pieces.append(piece)
    return pieces


def in_vmem(arrays):
    return [pltpu.with_memory_space_constraint(x, pltpu.VMEM) for x in arrays]


def middle_kernel(arrived, both, sent, kept):
    own = kept.shape[0]
    side, place = lax.axis_index("pair"), lax.axis_index("tp")
    total = both[side].astype(f32)
    added = arrived[0].astype(f32)
    for source in range(1, arrived.shape[0]):
        added = added + arrived[source].astype(f32)
    block = (total + added).astype(bf16)
    for target in range(sent.shape[0]):
        sent[target] = block
    block = block.astype(f32)
    chosen = jnp.zeros(kept.shape, f32)
    for n in range(block.shape[0] // own):
        chosen = chosen + jnp.where(place == n, block[n * own : (n + 1) * own], 0.0)
    kept[...] = chosen


def middle_rows(arrived, both, near, own):
    _, block, rows = both.shape
    arrived = pltpu.with_memory_space_constraint(arrived, pltpu.VMEM)
    both = pltpu.with_memory_space_constraint(both, pltpu.VMEM)
    return pl.pallas_call(
        middle_kernel,
        out_shape=(pltpu.VMEM((near, block, rows), bf16), pltpu.VMEM((own, rows), f32)),
    )(arrived, both)


def up_kernel(middle, *refs):
    pieces, sent = refs[:-1], refs[-1]
    me = lax.axis_index(LO)
    block = middle.shape[1]
    total, squares = 0.0, 0.0
    for step, piece in enumerate(pieces):
        part = middle[me ^ step]
        weight = jnp.transpose(piece[:block].astype(f32)).astype(bf16)
        total = total + dotted(weight, part, 1, 0)
        part = part.astype(f32)
        squares = squares + jnp.sum(part * part, axis=0, keepdims=True)
    tail = jnp.broadcast_to(squares, (8, squares.shape[1])).astype(bf16)
    share = total.shape[0] // sent.shape[0]
    for target in range(sent.shape[0]):
        sent[target, :share] = total[target * share : (target + 1) * share].astype(bf16)
        sent[target, share:] = tail


def up_sums(middle, pieces, far):
    middle = pltpu.with_memory_space_constraint(middle, pltpu.VMEM)
    share = pieces[0].shape[1] // far
    shape = (far, share + 8, middle.shape[2])
    return pl.pallas_call(up_kernel, out_shape=pltpu.VMEM(shape, bf16))(middle, *in_vmem(pieces))


def down_kernel(hidden, *refs):
    pieces, sent = refs[:-1], refs[-1]
    me = lax.axis_index(LO)
    own = sent.shape[1]
    whole = jnp.concatenate([hidden[n] for n in range(hidden.shape[0])], axis=0)
    for step, piece in enumerate(pieces):
        block = piece.shape[0] // 2
        part = dotted(piece[block:], whole, 1, 0)
        for n in range(block // own):
            sent[(me ^ step) * (block // own) + n] = part[n * own : (n + 1) * own].astype(bf16)


def down_sums(hidden, pieces, own):
    hidden = pltpu.with_memory_space_constraint(hidden, pltpu.VMEM)
    slots = len(pieces) * pieces[0].shape[0] // 2 // own
    shape = jax.ShapeDtypeStruct((slots, own, hidden.shape[2]), bf16)
    return pl.pallas_call(down_kernel, out_shape=shape)(hidden, *in_vmem(pieces))


def local(
    tokens,
    state,
    norm_gain,
    w_query,
    w_key,
    w_value,
    w_beta,
    w_decay,
    a_log,
    dt_bias,
    head_gain,
    w_out,
    mixer_gain,
    w_up,
    w_down,
):
    seq_here, heads_here, head_size = state.shape[:3]
    n_kv = lax.axis_size(KV)
    n_tp = lax.axis_size("tp")
    n_near = lax.axis_size(LO)
    width = w_beta.shape[0]
    rows, own = tokens.shape
    block = own * n_tp
    columns = heads_here * head_size
    assert heads_here == lax.axis_size("pair")

    tokens_t = tokens.T
    kept, given, gates = projection_weights(
        w_query, w_key, w_value, norm_gain, w_beta, w_decay, head_size
    )
    taken = lax.ppermute(given, "pair", [(0, 1), (1, 0)])

    both = from_everyone(tokens_t, ("pair", "tp")).reshape(2, block, rows)
    sent = partial_sums(both, kept, taken, gates, n_kv, seq_here)
    pieces = mixer_pieces(w_up, w_down, mixer_gain)
    arrived = exchange(sent, KV)
    arrived, pieces[0] = lax.optimization_barrier((arrived, pieces[0]))
    normed_all, keyed, fresh, decay = delta_update(
        arrived, state, a_log, dt_bias, head_gain, width, w_beta.shape[1]
    )
    every = exchange(normed_all, KV).reshape(rows, columns)
    new_state = state_update(state, keyed, fresh, decay)
    head_part = dotted(w_out, every, 0, 1).astype(bf16)
    arrived = from_everyone(head_part, "tp")
    middle_sent, middle_own = middle_rows(arrived, both, n_near, own)
    middle_sent, *pieces = lax.optimization_barrier((middle_sent, *pieces))
    middle = exchange(middle_sent, LO)
    sent = up_sums(middle, pieces, lax.axis_size("hi"))
    sums = exchange(sent, "hi").astype(f32).sum(axis=0)
    second = lax.rsqrt(sums[-1:] / width + epsilon)
    hidden_own = jnp.square(jax.nn.relu(second * sums[:-8])).astype(bf16)
    hidden = from_everyone(hidden_own, "hi")
    sent = down_sums(hidden, pieces, own)
    lowered = exchange(sent, NEAR).astype(f32).sum(axis=0)
    mixed = (middle_own + lowered).astype(bf16).T
    return (mixed, new_state)


def solution(mesh):
    near = min(NEIGHBOURS, mesh.shape["kv"])
    devices = mesh.devices.reshape(mesh.shape["grp"], -1, near // 2, 2, mesh.shape["tp"])
    fine = Mesh(devices, ("grp", *KV, "tp"))
    every = (*KV, "tp")
    return jax.shard_map(
        local,
        mesh=fine,
        in_specs=(
            P("grp", every),
            P(("grp", *KV), "tp", None, None),
            P(KV),
            P(KV, "tp"),
            P(KV, "tp"),
            P(KV, "tp"),
            P(),
            P(),
            P("tp"),
            P("tp"),
            P(),
            P("tp", KV),
            P(KV),
            P(KV, "tp"),
            P("tp", KV),
        ),
        out_specs=(P("grp", every), P(("grp", *KV), "tp", None, None)),
        check_vma=False,
    )
```

```python
import functools

import jax
import jax.numpy as jnp
from jax import lax
from jax.experimental import pallas as pl
from jax.experimental.pallas import tpu as pltpu
from jax.sharding import Mesh
from jax.sharding import PartitionSpec as P


epsilon = 1e-06
TAIL = 64
bf16 = jnp.bfloat16
f32 = jnp.float32
KV = ("hi", "mid", "pair")
LO = ("mid", "pair")
NEAR = (*LO, "tp")
NEIGHBOURS = 4


def exchange(x, axis):
    return lax.all_to_all(x, axis, split_axis=0, concat_axis=0, tiled=True)


def from_everyone(x, axis):
    return exchange(jnp.broadcast_to(x, (lax.axis_size(axis), *x.shape)), axis)


def dotted(left, right, left_dim, right_dim):
    dims = (((left_dim,), (right_dim,)), ((), ()))
    return lax.dot_general(left, right, dims, preferred_element_type=f32)


def delta_kernel(arrived, state, a_log, dt_bias, head_gain, normed_all, keyed_out, fresh_out, decay_out, *, width, all_heads):
    n_kv = arrived.shape[0]
    seq, heads = state.shape[:2]
    size = state.shape[3]
    main = 3 * size
    sums = []
    for head in range(heads):
        total = arrived[head].astype(f32)
        for source in range(head + heads, n_kv, heads):
            total = total + arrived[source].astype(f32)
        sums.append(total)
    ends = sums[0][:, 2 * main :]
    for total in sums[1:]:
        ends = ends + total[:, 2 * main :]
    gates = jnp.concatenate([ends[:, :TAIL], ends[:, TAIL:]], axis=0)
    sums = [jnp.concatenate([x[:, :main], x[:, main : 2 * main]], axis=0) for x in sums]
    tp_index = lax.axis_index("tp")
    lane = lax.broadcasted_iota(jnp.int32, gates.shape, 1)
    at = lambda n: jnp.sum(jnp.where(lane == n, gates, 0.0), axis=1, keepdims=True)
    first = lax.rsqrt(at(2 * all_heads) / width + epsilon)
    normed = []
    for head in range(heads):
        pre = first * sums[head]
        query, key, value = (pre[:, n * size : (n + 1) * size] for n in range(3))
        query = query * lax.rsqrt(jnp.sum(query * query, axis=1, keepdims=True) + epsilon)
        key = key * lax.rsqrt(jnp.sum(key * key, axis=1, keepdims=True) + epsilon)
        beta = jax.nn.sigmoid(first * at(heads * tp_index + head))
        logit = first * at(all_heads + heads * tp_index + head) + dt_bias[:, head : head + 1]
        soft = jnp.maximum(logit, 0.0) + jnp.log1p(jnp.exp(-jnp.abs(logit)))
        decay = jnp.exp(-jnp.exp(a_log[:, head : head + 1]) * soft)
        turned = jnp.transpose(jnp.concatenate([query, key], axis=0))
        reads = []
        for row in range(seq):
            matrix = state[row, head]
            reads.append(
                (
                    jnp.sum(matrix * turned[:, row : row + 1], axis=0, keepdims=True),
                    jnp.sum(matrix * turned[:, seq + row : seq + row + 1], axis=0, keepdims=True),
                )
            )
        query_read = jnp.concatenate([r[0] for r in reads], axis=0)
        key_read = jnp.concatenate([r[1] for r in reads], axis=0)
        fresh = beta * (value - decay * key_read)
        both = jnp.sum(query * key, axis=1, keepdims=True)
        reading = decay * query_read + both * fresh
        square = jnp.sum(reading * reading, axis=1, keepdims=True) / size
        normed.append(reading * lax.rsqrt(square + epsilon) * head_gain[...])
        keyed_out[head] = key
        fresh_out[head] = fresh
        decay_out[head] = jnp.broadcast_to(decay, (seq, size))
    whole = jnp.concatenate(normed, axis=1).astype(bf16)
    for target in range(n_kv):
        normed_all[target] = whole


def state_kernel(state, keyed, fresh, decay, new_state):
    seq, heads, _, _ = state.shape
    for head in range(heads):
        turned = jnp.transpose(jnp.concatenate([keyed[head], decay[head]], axis=0))
        for row in range(seq):
            column = turned[:, row : row + 1]
            scale = turned[:, seq + row : seq + row + 1]
            new_state[row, head] = scale * state[row, head] + column * fresh[head, row : row + 1, :]


def delta_update(arrived, state, a_log, dt_bias, head_gain, width, all_heads):
    n_kv = arrived.shape[0]
    seq, heads, size = state.shape[:3]
    small = pltpu.VMEM((heads, seq, size), f32)
    arrived = pltpu.with_memory_space_constraint(arrived, pltpu.VMEM)
    state = pltpu.with_memory_space_constraint(state, pltpu.VMEM)
    whole = pl.BlockSpec(memory_space=pltpu.VMEM)
    return pl.pallas_call(
        functools.partial(delta_kernel, width=width, all_heads=all_heads),
        in_specs=[whole] * 5,
        out_shape=(pltpu.VMEM((n_kv, seq, heads * size), bf16), small, small, small),
    )(arrived, state, a_log[None], dt_bias[None], head_gain[None])


def weights_kernel(*refs):
    sources, kept, given, gates, held, arrivals = refs[:6], refs[6], refs[7], refs[8], refs[9:15], refs[15]
    block = kept.shape[0]
    size = kept.shape[1] // 3
    side = lax.axis_index("pair")
    start = pl.multiple_of(lax.axis_index(KV[:2]) * (2 * block), 2 * block)
    copies = []
    for n, (source, target) in enumerate(zip(sources, held)):
        source = source.at[:, pl.ds(start, 2 * block)] if n >= 4 else source
        copies.append(pltpu.make_async_copy(source, target, arrivals.at[n]))
    for copy in copies:
        copy.start()
    for copy in copies:
        copy.wait()
    query, key, value, gain, beta, decay = held
    wide = gain[...].astype(f32)
    column = jnp.transpose(jnp.broadcast_to(wide, (8, block)))[:, :1]
    heads = []
    for head in range(2):
        cut = slice(head * size, (head + 1) * size)
        heads.append([w[:, cut].astype(f32) * column for w in (query, key, value)])
    for n in range(3):
        cut = slice(n * size, (n + 1) * size)
        kept[:, cut] = jnp.where(side == 0, heads[0][n], heads[1][n]).astype(bf16)
        given[:, cut] = jnp.where(side == 0, heads[1][n], heads[0][n]).astype(bf16)
    both = jnp.concatenate([beta[...].astype(f32), decay[...].astype(f32)], axis=0)
    both = jnp.where(side == 0, both[:, :block], both[:, block:])
    gates[...] = jnp.transpose(both * wide).astype(bf16)


def projection_weights(w_query, w_key, w_value, norm_gain, w_beta, w_decay, size):
    block = w_query.shape[0]
    assert 2 * block % 128 == 0
    sources = (w_query, w_key, w_value, norm_gain[None], w_beta.T, w_decay.T)
    held = [pltpu.VMEM(x.shape, bf16) for x in sources[:4]]
    held += [pltpu.VMEM((x.shape[0], 2 * block), bf16) for x in sources[4:]]
    cut = pltpu.VMEM((block, 3 * size), bf16)
    return pl.pallas_call(
        weights_kernel,
        in_specs=[pl.BlockSpec(memory_space=pl.ANY)] * 6,
        out_shape=(cut, cut, pltpu.VMEM((block, 2 * w_beta.shape[1]), bf16)),
        scratch_shapes=[*held, pltpu.SemaphoreType.DMA((6,))],
    )(*sources)


def sums_kernel(both, kept, taken, gates, sent):
    n_kv, half, _ = sent.shape
    side = lax.axis_index("pair")
    mine = jnp.transpose(both[side].astype(f32))
    other = jnp.transpose(both[1 - side].astype(f32))
    squares = jnp.sum(mine * mine, axis=1, keepdims=True)
    mine = mine.astype(bf16)
    main = dotted(mine, kept[...], 1, 0) + dotted(other.astype(bf16), taken[...], 1, 0)
    extra = dotted(mine, gates[...], 1, 0)
    gap = jnp.zeros((mine.shape[0], TAIL - extra.shape[1] - 1), f32)
    tail = jnp.concatenate([extra, squares, gap], axis=1)
    blank = jnp.zeros_like(tail)
    upper = jnp.concatenate([main, tail, blank], axis=1)
    lower = jnp.concatenate([blank, tail], axis=1)
    width = main.shape[1]
    for target in range(n_kv):
        at = 2 * target * half
        top, low = slice(at, at + half), slice(at + half, at + 2 * half)
        ends = upper[top, width:] + lower[low]
        sent[target] = jnp.concatenate([upper[top, :width], main[low], ends], axis=1).astype(bf16)


def partial_sums(both, kept, taken, gates, n_kv, seq):
    whole = pl.BlockSpec(memory_space=pltpu.VMEM)
    assert seq % 2 == 0 and gates.shape[1] < TAIL
    columns = 2 * (kept.shape[1] + TAIL)
    near = [pltpu.with_memory_space_constraint(x, pltpu.VMEM) for x in (both, kept, taken, gates)]
    return pl.pallas_call(
        sums_kernel,
        in_specs=[whole] * 4,
        out_shape=jax.ShapeDtypeStruct((n_kv, seq // 2, columns), bf16),
    )(*near)


def state_update(state, keyed, fresh, decay):
    small = [pltpu.with_memory_space_constraint(x, pltpu.VMEM) for x in (keyed, fresh, decay)]
    return pl.pallas_call(state_kernel, out_shape=jax.ShapeDtypeStruct(state.shape, f32))(state, *small)


def pieces_kernel(w_up, w_down_t, gain, *refs):
    near = lax.axis_size(LO)
    pieces, held, held_gain, arrivals = refs[:near], refs[near], refs[near + 1], refs[near + 2]
    me = lax.axis_index(LO)
    block = w_up.shape[0]
    share = pieces[0].shape[1]
    copies = [pltpu.make_async_copy(gain, held_gain, arrivals.at[2 * near])]
    for step, piece in enumerate(pieces):
        cut = pl.ds(pl.multiple_of((me ^ step) * share, share), share)
        copies.append(pltpu.make_async_copy(w_up.at[:, cut], held.at[step], arrivals.at[2 * step]))
        copies.append(
            pltpu.make_async_copy(w_down_t.at[:, cut], piece.at[pl.ds(block, block)], arrivals.at[2 * step + 1])
        )
    for copy in copies:
        copy.start()
    for copy in copies:
        copy.wait()
    wide = jnp.broadcast_to(held_gain[...].astype(f32), (8, block))
    column = jnp.transpose(wide)[:, :1]
    for step, piece in enumerate(pieces):
        piece[:block] = (held[step].astype(f32) * column).astype(bf16)


def mixer_pieces(w_up, w_down, mixer_gain):
    near = lax.axis_size(LO)
    block, wide = w_up.shape
    share = wide // near
    cut = pl.pallas_call(
        pieces_kernel,
        in_specs=[pl.BlockSpec(memory_space=pl.ANY)] * 3,
        out_shape=tuple(pltpu.VMEM((2 * block, share), bf16) for _ in range(near)),
        scratch_shapes=[
            pltpu.VMEM((near, block, share), bf16),
            pltpu.VMEM((1, block), bf16),
            pltpu.SemaphoreType.DMA((2 * near + 1,)),
        ],
    )(w_up, w_down.T, mixer_gain[None])
    pieces = []
    for step, piece in enumerate(cut):
        if step:
            piece = lax.ppermute(piece, LO, [(i, i ^ step) for i in range(near)])
        pieces.append(piece)
    return pieces


def in_vmem(arrays):
    return [pltpu.with_memory_space_constraint(x, pltpu.VMEM) for x in arrays]


def middle_kernel(arrived, both, sent, kept):
    own = kept.shape[0]
    side, place = lax.axis_index("pair"), lax.axis_index("tp")
    total = both[side].astype(f32)
    added = arrived[0].astype(f32)
    for source in range(1, arrived.shape[0]):
        added = added + arrived[source].astype(f32)
    block = (total + added).astype(bf16)
    for target in range(sent.shape[0]):
        sent[target] = block
    block = block.astype(f32)
    chosen = jnp.zeros(kept.shape, f32)
    for n in range(block.shape[0] // own):
        chosen = chosen + jnp.where(place == n, block[n * own : (n + 1) * own], 0.0)
    kept[...] = chosen


def middle_rows(arrived, both, near, own):
    _, block, rows = both.shape
    arrived = pltpu.with_memory_space_constraint(arrived, pltpu.VMEM)
    both = pltpu.with_memory_space_constraint(both, pltpu.VMEM)
    return pl.pallas_call(
        middle_kernel,
        out_shape=(pltpu.VMEM((near, block, rows), bf16), pltpu.VMEM((own, rows), f32)),
    )(arrived, both)


def up_kernel(middle, *refs):
    pieces, sent = refs[:-1], refs[-1]
    me = lax.axis_index(LO)
    block = middle.shape[1]
    total, squares = 0.0, 0.0
    for step, piece in enumerate(pieces):
        part = middle[me ^ step]
        weight = jnp.transpose(piece[:block].astype(f32)).astype(bf16)
        total = total + dotted(weight, part, 1, 0)
        part = part.astype(f32)
        squares = squares + jnp.sum(part * part, axis=0, keepdims=True)
    tail = jnp.broadcast_to(squares, (8, squares.shape[1])).astype(bf16)
    share = total.shape[0] // sent.shape[0]
    for target in range(sent.shape[0]):
        sent[target, :share] = total[target * share : (target + 1) * share].astype(bf16)
        sent[target, share:] = tail


def up_sums(middle, pieces, far):
    middle = pltpu.with_memory_space_constraint(middle, pltpu.VMEM)
    share = pieces[0].shape[1] // far
    shape = (far, share + 8, middle.shape[2])
    return pl.pallas_call(up_kernel, out_shape=pltpu.VMEM(shape, bf16))(middle, *in_vmem(pieces))


def down_kernel(hidden, *refs):
    pieces, sent = refs[:-1], refs[-1]
    me = lax.axis_index(LO)
    own = sent.shape[1]
    whole = jnp.concatenate([hidden[n] for n in range(hidden.shape[0])], axis=0)
    for step, piece in enumerate(pieces):
        block = piece.shape[0] // 2
        part = dotted(piece[block:], whole, 1, 0)
        for n in range(block // own):
            sent[(me ^ step) * (block // own) + n] = part[n * own : (n + 1) * own].astype(bf16)


def down_sums(hidden, pieces, own):
    hidden = pltpu.with_memory_space_constraint(hidden, pltpu.VMEM)
    slots = len(pieces) * pieces[0].shape[0] // 2 // own
    shape = jax.ShapeDtypeStruct((slots, own, hidden.shape[2]), bf16)
    return pl.pallas_call(down_kernel, out_shape=shape)(hidden, *in_vmem(pieces))


def local(
    tokens,
    state,
    norm_gain,
    w_query,
    w_key,
    w_value,
    w_beta,
    w_decay,
    a_log,
    dt_bias,
    head_gain,
    w_out,
    mixer_gain,
    w_up,
    w_down,
):
    seq_here, heads_here, head_size = state.shape[:3]
    n_kv = lax.axis_size(KV)
    n_tp = lax.axis_size("tp")
    n_near = lax.axis_size(LO)
    width = w_beta.shape[0]
    rows, own = tokens.shape
    block = own * n_tp
    columns = heads_here * head_size
    assert heads_here == lax.axis_size("pair")

    tokens_t = tokens.T
    kept, given, gates = projection_weights(
        w_query, w_key, w_value, norm_gain, w_beta, w_decay, head_size
    )
    taken = lax.ppermute(given, "pair", [(0, 1), (1, 0)])

    both = from_everyone(tokens_t, ("pair", "tp")).reshape(2, block, rows)
    sent = partial_sums(both, kept, taken, gates, n_kv, seq_here)
    pieces = mixer_pieces(w_up, w_down, mixer_gain)
    arrived = exchange(sent, KV)
    arrived, pieces[0] = lax.optimization_barrier((arrived, pieces[0]))
    normed_all, keyed, fresh, decay = delta_update(
        arrived, state, a_log, dt_bias, head_gain, width, w_beta.shape[1]
    )
    every = exchange(normed_all, KV).reshape(rows, columns)
    new_state = state_update(state, keyed, fresh, decay)
    head_part = dotted(w_out, every, 0, 1).astype(bf16)
    arrived = from_everyone(head_part, "tp")
    middle_sent, middle_own = middle_rows(arrived, both, n_near, own)
    middle_sent, *pieces = lax.optimization_barrier((middle_sent, *pieces))
    middle = exchange(middle_sent, LO)
    sent = up_sums(middle, pieces, lax.axis_size("hi"))
    sums = exchange(sent, "hi").astype(f32).sum(axis=0)
    second = lax.rsqrt(sums[-1:] / width + epsilon)
    hidden_own = jnp.square(jax.nn.relu(second * sums[:-8])).astype(bf16)
    hidden = from_everyone(hidden_own, "hi")
    sent = down_sums(hidden, pieces, own)
    lowered = exchange(sent, NEAR).astype(f32).sum(axis=0)
    mixed = (middle_own + lowered).astype(bf16).T
    return (mixed, new_state)


def solution(mesh):
    near = min(NEIGHBOURS, mesh.shape["kv"])
    devices = mesh.devices.reshape(mesh.shape["grp"], -1, near // 2, 2, mesh.shape["tp"])
    fine = Mesh(devices, ("grp", *KV, "tp"))
    every = (*KV, "tp")
    return jax.shard_map(
        local,
        mesh=fine,
        in_specs=(
            P("grp", every),
            P(("grp", *KV), "tp", None, None),
            P(KV),
            P(KV, "tp"),
            P(KV, "tp"),
            P(KV, "tp"),
            P(),
            P(),
            P("tp"),
            P("tp"),
            P(),
            P("tp", KV),
            P(KV),
            P(KV, "tp"),
            P("tp", KV),
        ),
        out_specs=(P("grp", every), P(("grp", *KV), "tp", None, None)),
        check_vma=False,
    )
```

```python
import functools

import jax
import jax.numpy as jnp
from jax import lax
from jax.experimental import pallas as pl
from jax.experimental.pallas import tpu as pltpu
from jax.sharding import Mesh
from jax.sharding import PartitionSpec as P


epsilon = 1e-06
TAIL = 64
bf16 = jnp.bfloat16
f32 = jnp.float32
KV = ("hi", "mid", "pair")
LO = ("mid", "pair")
NEAR = (*LO, "tp")
NEIGHBOURS = 4


def exchange(x, axis):
    return lax.all_to_all(x, axis, split_axis=0, concat_axis=0, tiled=True)


def from_everyone(x, axis):
    return exchange(jnp.broadcast_to(x, (lax.axis_size(axis), *x.shape)), axis)


def dotted(left, right, left_dim, right_dim):
    dims = (((left_dim,), (right_dim,)), ((), ()))
    return lax.dot_general(left, right, dims, preferred_element_type=f32)


def delta_kernel(arrived, state, a_log, dt_bias, head_gain, normed_all, keyed_out, fresh_out, decay_out, *, width, all_heads):
    n_kv = arrived.shape[0]
    seq, heads = state.shape[:2]
    size = state.shape[3]
    main = 3 * size
    sums = []
    for head in range(heads):
        total = arrived[head].astype(f32)
        for source in range(head + heads, n_kv, heads):
            total = total + arrived[source].astype(f32)
        sums.append(total)
    ends = sums[0][:, 2 * main :]
    for total in sums[1:]:
        ends = ends + total[:, 2 * main :]
    gates = jnp.concatenate([ends[:, :TAIL], ends[:, TAIL:]], axis=0)
    sums = [jnp.concatenate([x[:, :main], x[:, main : 2 * main]], axis=0) for x in sums]
    tp_index = lax.axis_index("tp")
    lane = lax.broadcasted_iota(jnp.int32, gates.shape, 1)
    at = lambda n: jnp.sum(jnp.where(lane == n, gates, 0.0), axis=1, keepdims=True)
    first = lax.rsqrt(at(2 * all_heads) / width + epsilon)
    normed = []
    for head in range(heads):
        pre = first * sums[head]
        query, key, value = (pre[:, n * size : (n + 1) * size] for n in range(3))
        query = query * lax.rsqrt(jnp.sum(query * query, axis=1, keepdims=True) + epsilon)
        key = key * lax.rsqrt(jnp.sum(key * key, axis=1, keepdims=True) + epsilon)
        beta = jax.nn.sigmoid(first * at(heads * tp_index + head))
        logit = first * at(all_heads + heads * tp_index + head) + dt_bias[:, head : head + 1]
        soft = jnp.maximum(logit, 0.0) + jnp.log1p(jnp.exp(-jnp.abs(logit)))
        decay = jnp.exp(-jnp.exp(a_log[:, head : head + 1]) * soft)
        turned = jnp.transpose(jnp.concatenate([query, key], axis=0))
        reads = []
        for row in range(seq):
            matrix = state[row, head]
            reads.append(
                (
                    jnp.sum(matrix * turned[:, row : row + 1], axis=0, keepdims=True),
                    jnp.sum(matrix * turned[:, seq + row : seq + row + 1], axis=0, keepdims=True),
                )
            )
        query_read = jnp.concatenate([r[0] for r in reads], axis=0)
        key_read = jnp.concatenate([r[1] for r in reads], axis=0)
        fresh = beta * (value - decay * key_read)
        both = jnp.sum(query * key, axis=1, keepdims=True)
        reading = decay * query_read + both * fresh
        square = jnp.sum(reading * reading, axis=1, keepdims=True) / size
        normed.append(reading * lax.rsqrt(square + epsilon) * head_gain[...])
        keyed_out[head] = key
        fresh_out[head] = fresh
        decay_out[head] = jnp.broadcast_to(decay, (seq, size))
    whole = jnp.concatenate(normed, axis=1).astype(bf16)
    for target in range(n_kv):
        normed_all[target] = whole


def state_kernel(state, keyed, fresh, decay, new_state):
    seq, heads, _, _ = state.shape
    for head in range(heads):
        turned = jnp.transpose(jnp.concatenate([keyed[head], decay[head]], axis=0))
        for row in range(seq):
            column = turned[:, row : row + 1]
            scale = turned[:, seq + row : seq + row + 1]
            new_state[row, head] = scale * state[row, head] + column * fresh[head, row : row + 1, :]


def delta_update(arrived, state, a_log, dt_bias, head_gain, width, all_heads):
    n_kv = arrived.shape[0]
    seq, heads, size = state.shape[:3]
    small = pltpu.VMEM((heads, seq, size), f32)
    arrived = pltpu.with_memory_space_constraint(arrived, pltpu.VMEM)
    state = pltpu.with_memory_space_constraint(state, pltpu.VMEM)
    whole = pl.BlockSpec(memory_space=pltpu.VMEM)
    return pl.pallas_call(
        functools.partial(delta_kernel, width=width, all_heads=all_heads),
        in_specs=[whole] * 5,
        out_shape=(pltpu.VMEM((n_kv, seq, heads * size), bf16), small, small, small),
    )(arrived, state, a_log[None], dt_bias[None], head_gain[None])


def weights_kernel(*refs):
    sources, kept, given, gates, held, arrivals = refs[:6], refs[6], refs[7], refs[8], refs[9:15], refs[15]
    block = kept.shape[0]
    size = kept.shape[1] // 3
    side = lax.axis_index("pair")
    start = pl.multiple_of(lax.axis_index(KV[:2]) * (2 * block), 2 * block)
    copies = []
    for n, (source, target) in enumerate(zip(sources, held)):
        source = source.at[:, pl.ds(start, 2 * block)] if n >= 4 else source
        copies.append(pltpu.make_async_copy(source, target, arrivals.at[n]))
    for copy in copies:
        copy.start()
    for copy in copies:
        copy.wait()
    query, key, value, gain, beta, decay = held
    wide = gain[...].astype(f32)
    column = jnp.transpose(jnp.broadcast_to(wide, (8, block)))[:, :1]
    heads = []
    for head in range(2):
        cut = slice(head * size, (head + 1) * size)
        heads.append([w[:, cut].astype(f32) * column for w in (query, key, value)])
    for n in range(3):
        cut = slice(n * size, (n + 1) * size)
        kept[:, cut] = jnp.where(side == 0, heads[0][n], heads[1][n]).astype(bf16)
        given[:, cut] = jnp.where(side == 0, heads[1][n], heads[0][n]).astype(bf16)
    both = jnp.concatenate([beta[...].astype(f32), decay[...].astype(f32)], axis=0)
    both = jnp.where(side == 0, both[:, :block], both[:, block:])
    gates[...] = jnp.transpose(both * wide).astype(bf16)


def projection_weights(w_query, w_key, w_value, norm_gain, w_beta, w_decay, size):
    block = w_query.shape[0]
    assert 2 * block % 128 == 0
    sources = (w_query, w_key, w_value, norm_gain[None], w_beta.T, w_decay.T)
    held = [pltpu.VMEM(x.shape, bf16) for x in sources[:4]]
    held += [pltpu.VMEM((x.shape[0], 2 * block), bf16) for x in sources[4:]]
    cut = pltpu.VMEM((block, 3 * size), bf16)
    return pl.pallas_call(
        weights_kernel,
        in_specs=[pl.BlockSpec(memory_space=pl.ANY)] * 6,
        out_shape=(cut, cut, pltpu.VMEM((block, 2 * w_beta.shape[1]), bf16)),
        scratch_shapes=[*held, pltpu.SemaphoreType.DMA((6,))],
    )(*sources)


def own_kernel(both, kept, gates, main, tail):
    mine = jnp.transpose(both[lax.axis_index("pair")].astype(f32))
    squares = jnp.sum(mine * mine, axis=1, keepdims=True)
    mine = mine.astype(bf16)
    main[...] = dotted(mine, kept[...], 1, 0)
    extra = dotted(mine, gates[...], 1, 0)
    gap = jnp.zeros((mine.shape[0], TAIL - extra.shape[1] - 1), f32)
    tail[...] = jnp.concatenate([extra, squares, gap], axis=1)


def own_sums(both, kept, gates):
    rows = both.shape[2]
    out = (pltpu.VMEM((rows, kept.shape[1]), f32), pltpu.VMEM((rows, TAIL), f32))
    return pl.pallas_call(own_kernel, out_shape=out)(*in_vmem((both, kept, gates)))


def sums_kernel(both, taken, own_main, own_tail, sent):
    n_kv, half, _ = sent.shape
    other = jnp.transpose(both[1 - lax.axis_index("pair")].astype(f32)).astype(bf16)
    main = own_main[...] + dotted(other, taken[...], 1, 0)
    tail = own_tail[...]
    blank = jnp.zeros_like(tail)
    upper = jnp.concatenate([main, tail, blank], axis=1)
    lower = jnp.concatenate([blank, tail], axis=1)
    width = main.shape[1]
    for target in range(n_kv):
        at = 2 * target * half
        top, low = slice(at, at + half), slice(at + half, at + 2 * half)
        ends = upper[top, width:] + lower[low]
        sent[target] = jnp.concatenate([upper[top, :width], main[low], ends], axis=1).astype(bf16)


def partial_sums(both, taken, main, tail, n_kv, seq):
    assert seq % 2 == 0
    shape = (n_kv, seq // 2, 2 * (main.shape[1] + TAIL))
    near = in_vmem((both, taken, main, tail))
    return pl.pallas_call(sums_kernel, out_shape=jax.ShapeDtypeStruct(shape, bf16))(*near)


def state_update(state, keyed, fresh, decay):
    small = [pltpu.with_memory_space_constraint(x, pltpu.VMEM) for x in (keyed, fresh, decay)]
    return pl.pallas_call(state_kernel, out_shape=jax.ShapeDtypeStruct(state.shape, f32))(state, *small)


def pieces_kernel(w_up, w_down_t, gain, *refs):
    near = lax.axis_size(LO)
    pieces, held, held_gain, arrivals = refs[:near], refs[near], refs[near + 1], refs[near + 2]
    me = lax.axis_index(LO)
    block = w_up.shape[0]
    share = pieces[0].shape[1]
    copies = [pltpu.make_async_copy(gain, held_gain, arrivals.at[2 * near])]
    for step, piece in enumerate(pieces):
        cut = pl.ds(pl.multiple_of((me ^ step) * share, share), share)
        copies.append(pltpu.make_async_copy(w_up.at[:, cut], held.at[step], arrivals.at[2 * step]))
        copies.append(
            pltpu.make_async_copy(w_down_t.at[:, cut], piece.at[pl.ds(block, block)], arrivals.at[2 * step + 1])
        )
    for copy in copies:
        copy.start()
    for copy in copies:
        copy.wait()
    wide = jnp.broadcast_to(held_gain[...].astype(f32), (8, block))
    column = jnp.transpose(wide)[:, :1]
    for step, piece in enumerate(pieces):
        piece[:block] = (held[step].astype(f32) * column).astype(bf16)


def mixer_pieces(w_up, w_down, mixer_gain):
    near = lax.axis_size(LO)
    block, wide = w_up.shape
    share = wide // near
    cut = pl.pallas_call(
        pieces_kernel,
        in_specs=[pl.BlockSpec(memory_space=pl.ANY)] * 3,
        out_shape=tuple(pltpu.VMEM((2 * block, share), bf16) for _ in range(near)),
        scratch_shapes=[
            pltpu.VMEM((near, block, share), bf16),
            pltpu.VMEM((1, block), bf16),
            pltpu.SemaphoreType.DMA((2 * near + 1,)),
        ],
    )(w_up, w_down.T, mixer_gain[None])
    pieces = []
    for step, piece in enumerate(cut):
        if step:
            piece = lax.ppermute(piece, LO, [(i, i ^ step) for i in range(near)])
        pieces.append(piece)
    return pieces


def in_vmem(arrays):
    return [pltpu.with_memory_space_constraint(x, pltpu.VMEM) for x in arrays]


def middle_kernel(arrived, both, sent, kept):
    own = kept.shape[0]
    side, place = lax.axis_index("pair"), lax.axis_index("tp")
    total = both[side].astype(f32)
    added = arrived[0].astype(f32)
    for source in range(1, arrived.shape[0]):
        added = added + arrived[source].astype(f32)
    block = (total + added).astype(bf16)
    for target in range(sent.shape[0]):
        sent[target] = block
    block = block.astype(f32)
    chosen = jnp.zeros(kept.shape, f32)
    for n in range(block.shape[0] // own):
        chosen = chosen + jnp.where(place == n, block[n * own : (n + 1) * own], 0.0)
    kept[...] = chosen


def middle_rows(arrived, both, near, own):
    _, block, rows = both.shape
    arrived = pltpu.with_memory_space_constraint(arrived, pltpu.VMEM)
    both = pltpu.with_memory_space_constraint(both, pltpu.VMEM)
    return pl.pallas_call(
        middle_kernel,
        out_shape=(pltpu.VMEM((near, block, rows), bf16), pltpu.VMEM((own, rows), f32)),
    )(arrived, both)


def up_kernel(middle, *refs):
    pieces, sent = refs[:-1], refs[-1]
    me = lax.axis_index(LO)
    block = middle.shape[1]
    total, squares = 0.0, 0.0
    for step, piece in enumerate(pieces):
        part = middle[me ^ step]
        weight = jnp.transpose(piece[:block].astype(f32)).astype(bf16)
        total = total + dotted(weight, part, 1, 0)
        part = part.astype(f32)
        squares = squares + jnp.sum(part * part, axis=0, keepdims=True)
    tail = jnp.broadcast_to(squares, (8, squares.shape[1])).astype(bf16)
    share = total.shape[0] // sent.shape[0]
    for target in range(sent.shape[0]):
        sent[target, :share] = total[target * share : (target + 1) * share].astype(bf16)
        sent[target, share:] = tail


def up_sums(middle, pieces, far):
    middle = pltpu.with_memory_space_constraint(middle, pltpu.VMEM)
    share = pieces[0].shape[1] // far
    shape = (far, share + 8, middle.shape[2])
    return pl.pallas_call(up_kernel, out_shape=pltpu.VMEM(shape, bf16))(middle, *in_vmem(pieces))


def down_kernel(hidden, *refs):
    pieces, sent = refs[:-1], refs[-1]
    me = lax.axis_index(LO)
    own = sent.shape[1]
    whole = jnp.concatenate([hidden[n] for n in range(hidden.shape[0])], axis=0)
    for step, piece in enumerate(pieces):
        block = piece.shape[0] // 2
        part = dotted(piece[block:], whole, 1, 0)
        for n in range(block // own):
            sent[(me ^ step) * (block // own) + n] = part[n * own : (n + 1) * own].astype(bf16)


def down_sums(hidden, pieces, own):
    hidden = pltpu.with_memory_space_constraint(hidden, pltpu.VMEM)
    slots = len(pieces) * pieces[0].shape[0] // 2 // own
    shape = jax.ShapeDtypeStruct((slots, own, hidden.shape[2]), bf16)
    return pl.pallas_call(down_kernel, out_shape=shape)(hidden, *in_vmem(pieces))


def local(
    tokens,
    state,
    norm_gain,
    w_query,
    w_key,
    w_value,
    w_beta,
    w_decay,
    a_log,
    dt_bias,
    head_gain,
    w_out,
    mixer_gain,
    w_up,
    w_down,
):
    seq_here, heads_here, head_size = state.shape[:3]
    n_kv = lax.axis_size(KV)
    n_tp = lax.axis_size("tp")
    n_near = lax.axis_size(LO)
    width = w_beta.shape[0]
    rows, own = tokens.shape
    block = own * n_tp
    columns = heads_here * head_size
    assert heads_here == lax.axis_size("pair")

    tokens_t = tokens.T
    kept, given, gates = projection_weights(
        w_query, w_key, w_value, norm_gain, w_beta, w_decay, head_size
    )
    taken = lax.ppermute(given, "pair", [(0, 1), (1, 0)])

    both = from_everyone(tokens_t, ("pair", "tp")).reshape(2, block, rows)
    main, tail = own_sums(both, kept, gates)
    sent = partial_sums(both, taken, main, tail, n_kv, seq_here)
    pieces = mixer_pieces(w_up, w_down, mixer_gain)
    arrived = exchange(sent, KV)
    arrived, pieces[0] = lax.optimization_barrier((arrived, pieces[0]))
    normed_all, keyed, fresh, decay = delta_update(
        arrived, state, a_log, dt_bias, head_gain, width, w_beta.shape[1]
    )
    every = exchange(normed_all, KV).reshape(rows, columns)
    new_state = state_update(state, keyed, fresh, decay)
    head_part = dotted(w_out, every, 0, 1).astype(bf16)
    arrived = from_everyone(head_part, "tp")
    middle_sent, middle_own = middle_rows(arrived, both, n_near, own)
    middle_sent, *pieces = lax.optimization_barrier((middle_sent, *pieces))
    middle = exchange(middle_sent, LO)
    sent = up_sums(middle, pieces, lax.axis_size("hi"))
    sums = exchange(sent, "hi").astype(f32).sum(axis=0)
    second = lax.rsqrt(sums[-1:] / width + epsilon)
    hidden_own = jnp.square(jax.nn.relu(second * sums[:-8])).astype(bf16)
    hidden = from_everyone(hidden_own, "hi")
    sent = down_sums(hidden, pieces, own)
    lowered = exchange(sent, NEAR).astype(f32).sum(axis=0)
    mixed = (middle_own + lowered).astype(bf16).T
    return (mixed, new_state)


def solution(mesh):
    near = min(NEIGHBOURS, mesh.shape["kv"])
    devices = mesh.devices.reshape(mesh.shape["grp"], -1, near // 2, 2, mesh.shape["tp"])
    fine = Mesh(devices, ("grp", *KV, "tp"))
    every = (*KV, "tp")
    return jax.shard_map(
        local,
        mesh=fine,
        in_specs=(
            P("grp", every),
            P(("grp", *KV), "tp", None, None),
            P(KV),
            P(KV, "tp"),
            P(KV, "tp"),
            P(KV, "tp"),
            P(),
            P(),
            P("tp"),
            P("tp"),
            P(),
            P("tp", KV),
            P(KV),
            P(KV, "tp"),
            P("tp", KV),
        ),
        out_specs=(P("grp", every), P(("grp", *KV), "tp", None, None)),
        check_vma=False,
    )
```
